1024 devices in a mesh: ep: 64 (over z, y), tp: 16 (over x, core).
Axes of the slice: x: 8, y: 8, z: 8, core: 2. Of those that a mesh axis runs over, the one named last changes fastest.
Arguments:
- hidden: bfloat16 [1024, 2048], P('ep'), may hold values from -6 to 6
- lengths: int32 [1024], P(('ep', 'tp')), may hold values from 1 to 1535, 786432 in all
- latent_cache: bfloat16 [1024, 1536, 512], P(('ep', 'tp')), may hold values from -6 to 6
- cache_rotary: bfloat16 [1024, 32, 1536], P(('ep', 'tp')), may hold values from -1500 to 1500
- attn_gain: bfloat16 [2048], replicated, may hold values from 0.099609375 to 1.8984375
- w_query_nope: bfloat16 [2048, 1024], P(None, 'tp'), may hold values from -0.125 to 0.125
- w_query_rope: bfloat16 [2048, 512], P(None, 'tp'), may hold values from -0.125 to 0.125
- latent_weight: bfloat16 [2048, 512], replicated, may hold values from -0.125 to 0.125
- w_rotary_key: bfloat16 [2048, 32], replicated, may hold values from -0.125 to 0.125
- latent_norm_gain: bfloat16 [512], replicated, may hold values from 0.099609375 to 1.8984375
- key_up_weight: bfloat16 [1024, 512], P('tp'), may hold values from -0.75 to 0.75
- value_up_weight: bfloat16 [512, 1024], P(None, 'tp'), may hold values from -0.25 to 0.25
- head_gain: bfloat16 [1024], P('tp'), may hold values from 0.099609375 to 1.8984375
- w_output: bfloat16 [1024, 2048], P('tp'), may hold values from -0.1875 to 0.1875
- ffn_gain: bfloat16 [2048], replicated, may hold values from 0.099609375 to 1.8984375
- expert_ids: int32 [1024, 4], P('ep'), may hold values from 0 to 63, all different within a row; in each aligned block of 16 rows (0 to 15, 16 to 31, ...) at most 2 rows name the same one
- expert_weights: float32 [1024, 4], P('ep'), may hold values from 0.2 to 1.2
- w_expert_gate: bfloat16 [64, 2048, 2048], P('ep', None, 'tp'), may hold values from -0.125 to 0.125
- w_expert_up: bfloat16 [64, 2048, 2048], P('ep', None, 'tp'), may hold values from -0.125 to 0.125
- w_expert_down: bfloat16 [64, 2048, 2048], P('ep', 'tp'), may hold values from -0.125 to 0.125
- w_shared_gate: bfloat16 [2048, 1024], P(None, 'tp'), may hold values from -0.125 to 0.125
- w_shared_up: bfloat16 [2048, 1024], P(None, 'tp'), may hold values from -0.125 to 0.125
- w_shared_down: bfloat16 [1024, 2048], P('tp'), may hold values from -0.1875 to 0.1875
- w_dense_up: bfloat16 [2048, 2048], P(None, 'tp'), may hold values from -0.125 to 0.125
- w_dense_down: bfloat16 [2048, 2048], P('tp'), may hold values from -0.125 to 0.125
- dense_gate: bfloat16 [2048], replicated, may hold values from -0.125 to 0.125
Outputs:
- layer_out: bfloat16 [1024, 2048], P('ep', 'tp')
The draws below stay inside these ranges and needn't reach their ends.
Inputs may be any that keep to these rules, and one draw needn't show every extreme that they name: `lengths`: past positions of each sequence; the longest has exactly 1535, so every cache has room for the new token. `expert_ids`: A row's 4 experts differ. Among the rows of one index of ep (16 rows), no expert is named by more than 2 of them, a bound that some block reaches.
All inputs are finite; a program needn't handle non-finite values. No bound on the sum of `lengths` on one device may be relied on, other than what follows from the above.
Results may differ from the reference program's by a relative error of at most 0.024.
Values may be sent and summed in bfloat16 or wider, within the bound.
No kernel may reach another device: no remote copies, remote signals or barrier semaphores. Data moves between devices by JAX's collectives and lax.ppermute only.
A program may use at most 32 MiB of HBM per device.

```python
import math
import jax
import jax.numpy as jnp
import numpy as np
from jax import lax

MODEL_WIDTH = 2048
HEAD_COUNT = 16
PLAIN_QUERY = 64
ROPE = 32
VALUE_UNITS = 64
LATENT_UNITS = 512
E_FF = 2048
S_FF = 1024
DENSE_FF = 2048
TOPK = 4
CACHE_LENGTH = 1536
SEQ_GRP = 16
SEQUENCE_COUNT = 1024
EXPERTS = 64
CAP = 2
N_EP = 64
N_TP = 16


def draw_cache_rotary(key, part):
    base_key = jax.random.fold_in(key, 11)
    values = jnp.clip(jax.random.normal(base_key, (SEQUENCE_COUNT, ROPE, CACHE_LENGTH), jnp.float32), -6.0, 6.0)
    return values.astype(jnp.bfloat16)


def shard_levels(key, extent, pieces, smallest, top_value):
    def one(position, parts):
        heights = jax.random.uniform(jax.random.fold_in(jax.random.fold_in(key, 6), position), (parts,), jnp.float32, smallest / len(pieces), top_value / len(pieces))
        return jnp.repeat(jnp.exp(heights), extent[position] // parts).reshape((-1,) + (1,) * (len(extent) - position - 1))

    factor_of = one(*pieces[0])
    for cut in pieces[1:]:
        factor_of = factor_of * one(*cut)
    return factor_of


def split_up(count, total, limit, lean):
    portions = [(1 << 20) // math.isqrt(grade ** lean) + 1 for grade in range(2, count + 1)]
    spare, counts = total - limit - (count - 1), [1] * (count - 1)
    while spare > 0:
        candidates = [i for i in range(count - 1) if counts[i] < limit]
        whole, left = sum([portions[i] for i in candidates]), spare
        for i in candidates:
            addition = min(limit - counts[i], max(1, left * portions[i] // whole), spare)
            counts[i] = counts[i] + addition
            spare = spare - addition
    return np.array([limit] + counts)


def ragged_sizes(key, count, total, bound, slope):
    if count == 2:
        one = jax.random.randint(key, (), max(1, total - bound), min(bound, total - 1) + 1)
        return jnp.stack([one, total - one])
    sizes = jnp.asarray(split_up(count, total, bound, slope), jnp.int32)
    pairs = (count - 1) // 2
    source_of, receiver = sizes[1:1 + 2 * pairs:2], sizes[2:2 + 2 * pairs:2]
    slack = jnp.minimum(source_of - 1, bound - receiver)
    shifted = jax.random.randint(jax.random.fold_in(key, 1), (pairs,), 0, 1 << 20) % (slack + 1)
    sizes = sizes.at[1:1 + 2 * pairs:2].set(source_of - shifted).at[2:2 + 2 * pairs:2].set(receiver + shifted)
    return sizes[jax.random.permutation(jax.random.fold_in(key, 2), count)]


def deal_out(rng, own, number, rows, count, top, limit, skew):
    ranking = jax.random.permutation(rng, count)
    heavy_load, ordinary = load_shares(count, rows * top, limit, skew, True), load_shares(count, rows * top, limit, skew, False)
    places = jnp.arange(count)

    def named(sizes, rotation):
        used = int((sizes > 0).sum())
        fixed = max(1, used // 4)
        passed = fixed + (places - fixed + rotation * (used - fixed)) % max(1, count - fixed)
        return jnp.zeros((count,), jnp.int32).at[ranking[jnp.where(places < fixed, places, passed)]].set(jnp.asarray(sizes, jnp.int32))

    sizes = jnp.where(number % 4 == 0, named(heavy_load, number // 4), named(ordinary, number - number // 4 - 1))
    mixed = jax.random.permutation(jax.random.fold_in(own, 3), count)
    source_of, receiver = mixed[0:count // 2 * 2:2], mixed[1:count // 2 * 2:2]
    slack = jnp.minimum(sizes[source_of] - 1, limit - sizes[receiver]) // 2
    slack = jnp.where((source_of == ranking[0]) | (receiver == ranking[0]) | (sizes[receiver] == 0), 0, jnp.maximum(slack, 0))
    passed = jax.random.randint(jax.random.fold_in(own, 4), (count // 2,), 0, 1 << 20) % (slack + 1)
    sizes = sizes.at[source_of].add(-passed).at[receiver].add(passed)
    items = jnp.searchsorted(jnp.cumsum(sizes), jnp.arange(rows * top), side="right").astype(jnp.int32)
    listing = items.reshape(top, rows).T
    listing = listing[jax.random.permutation(jax.random.fold_in(own, 1), rows)]
    rotation = jax.random.randint(jax.random.fold_in(own, 2), (rows, 1), 0, top)
    return jnp.take_along_axis(listing, (jnp.arange(top)[None, :] + rotation) % top, axis=1)


def load_shares(number_of, total, bound, skew, full):
    loads = [(1 << 20) // math.isqrt(standing ** skew) + 1 for standing in range(1, number_of + 1)]
    largest = bound if full else min(bound, max(-(-total // number_of), total * loads[0] // sum(loads)))
    least = 1 if total - largest >= number_of - 1 else 0
    counts, surplus = [largest] + [least] * (number_of - 1), total - largest - least * (number_of - 1)
    while surplus > 0:
        candidates = [i for i in range(1, number_of) if counts[i] < largest] or [i for i in range(1, number_of) if counts[i] < bound]
        mass, left = sum([loads[i] for i in candidates]), surplus
        for i in candidates:
            extra = min(bound - counts[i], max(1, left * loads[i] // mass), surplus)
            counts[i] = counts[i] + extra
            surplus = surplus - extra
    return np.array(counts)


def bell_draw(key, extent, deviation, bound, cuts=(), kind=jnp.bfloat16):
    values = deviation * jax.random.normal(key, extent, jnp.float32)
    if cuts:
        values = values * shard_levels(key, extent, cuts, -0.22, 0.18)
    return jnp.clip(values, -bound, bound).astype(kind)


def setup_inputs(seed: int = 0) -> dict:
    arg_keys = jax.random.split(jax.random.key(seed), 27)
    hidden = bell_draw(arg_keys[0], (SEQUENCE_COUNT, MODEL_WIDTH), 1.0, 6.0, ((0, 64),))
    lengths = ragged_sizes(arg_keys[1], SEQUENCE_COUNT, SEQUENCE_COUNT * CACHE_LENGTH // 2, CACHE_LENGTH - 1, 2).astype(jnp.int32)
    latent_cache = bell_draw(arg_keys[2], (SEQUENCE_COUNT, CACHE_LENGTH, LATENT_UNITS), 1.0, 6.0, ((0, 1024),))
    cache_rotary = draw_cache_rotary(jax.random.fold_in(arg_keys[26], 71), 0)
    attn_gain = jnp.clip(1.0 + 0.18 * jax.random.normal(arg_keys[4], (MODEL_WIDTH,), jnp.float32), 0.099609375, 1.8984375).astype(jnp.bfloat16)
    w_query_nope = bell_draw(arg_keys[5], (MODEL_WIDTH, HEAD_COUNT * PLAIN_QUERY), MODEL_WIDTH ** -0.5, 0.125, ((1, 16),))
    w_query_rope = bell_draw(arg_keys[6], (MODEL_WIDTH, HEAD_COUNT * ROPE), MODEL_WIDTH ** -0.5, 0.125, ((1, 16),))
    latent_weight = bell_draw(arg_keys[7], (MODEL_WIDTH, LATENT_UNITS), MODEL_WIDTH ** -0.5, 0.125)
    w_rotary_key = bell_draw(arg_keys[8], (MODEL_WIDTH, ROPE), MODEL_WIDTH ** -0.5, 0.125)
    latent_norm_gain = jnp.clip(1.0 + 0.18 * jax.random.normal(arg_keys[9], (LATENT_UNITS,), jnp.float32), 0.099609375, 1.8984375).astype(jnp.bfloat16)
    key_up_weight = bell_draw(arg_keys[10], (HEAD_COUNT * PLAIN_QUERY, LATENT_UNITS), PLAIN_QUERY ** -0.5, 0.75, ((0, 16),))
    value_up_weight = bell_draw(arg_keys[11], (LATENT_UNITS, HEAD_COUNT * VALUE_UNITS), LATENT_UNITS ** -0.5, 0.25, ((1, 16),))
    head_gain = jnp.clip(1.0 + 0.18 * jax.random.normal(arg_keys[12], (HEAD_COUNT * VALUE_UNITS,), jnp.float32), 0.099609375, 1.8984375).astype(jnp.bfloat16)
    w_output = bell_draw(arg_keys[13], (HEAD_COUNT * VALUE_UNITS, MODEL_WIDTH), (HEAD_COUNT * VALUE_UNITS) ** -0.5, 0.1875, ((0, 16),))
    ffn_gain = jnp.clip(1.0 + 0.18 * jax.random.normal(arg_keys[14], (MODEL_WIDTH,), jnp.float32), 0.099609375, 1.8984375).astype(jnp.bfloat16)
    expert_ids_keys = jax.random.split(jax.random.fold_in(arg_keys[15], 1), SEQUENCE_COUNT // SEQ_GRP)
    expert_ids_turns = jax.random.permutation(jax.random.fold_in(arg_keys[15], 3), SEQUENCE_COUNT // SEQ_GRP)
    expert_ids = jax.vmap(lambda own, number: deal_out(jax.random.fold_in(arg_keys[15], 2), own, number, SEQ_GRP, EXPERTS, TOPK, CAP, 2))(expert_ids_keys, expert_ids_turns).reshape((SEQUENCE_COUNT, TOPK))
    expert_weights = jnp.clip(0.2 + 1 * jax.random.uniform(arg_keys[16], (SEQUENCE_COUNT, TOPK), jnp.float32) ** shard_levels(arg_keys[16], (SEQUENCE_COUNT, TOPK), ((0, 64),), -0.2, 0.2), 0.2, 1.2)
    w_expert_gate = bell_draw(arg_keys[17], (EXPERTS, MODEL_WIDTH, E_FF), MODEL_WIDTH ** -0.5, 0.125, ((0, 64), (2, 16)))
    w_expert_up = bell_draw(arg_keys[18], (EXPERTS, MODEL_WIDTH, E_FF), MODEL_WIDTH ** -0.5, 0.125, ((0, 64), (2, 16)))
    w_expert_down = bell_draw(arg_keys[19], (EXPERTS, E_FF, MODEL_WIDTH), E_FF ** -0.5, 0.125, ((0, 64), (1, 16)))
    w_shared_gate = bell_draw(arg_keys[20], (MODEL_WIDTH, S_FF), MODEL_WIDTH ** -0.5, 0.125, ((1, 16),))
    w_shared_up = bell_draw(arg_keys[21], (MODEL_WIDTH, S_FF), MODEL_WIDTH ** -0.5, 0.125, ((1, 16),))
    w_shared_down = bell_draw(arg_keys[22], (S_FF, MODEL_WIDTH), S_FF ** -0.5, 0.1875, ((0, 16),))
    w_dense_up = bell_draw(arg_keys[23], (MODEL_WIDTH, DENSE_FF), MODEL_WIDTH ** -0.5, 0.125, ((1, 16),))
    w_dense_down = bell_draw(arg_keys[24], (DENSE_FF, MODEL_WIDTH), DENSE_FF ** -0.5, 0.125, ((0, 16),))
    dense_gate = bell_draw(arg_keys[25], (MODEL_WIDTH,), MODEL_WIDTH ** -0.5, 0.125)
    return {"hidden": hidden, "lengths": lengths, "latent_cache": latent_cache, "cache_rotary": cache_rotary, "attn_gain": attn_gain, "w_query_nope": w_query_nope, "w_query_rope": w_query_rope, "latent_weight": latent_weight, "w_rotary_key": w_rotary_key, "latent_norm_gain": latent_norm_gain, "key_up_weight": key_up_weight, "value_up_weight": value_up_weight, "head_gain": head_gain, "w_output": w_output, "ffn_gain": ffn_gain, "expert_ids": expert_ids, "expert_weights": expert_weights, "w_expert_gate": w_expert_gate, "w_expert_up": w_expert_up, "w_expert_down": w_expert_down, "w_shared_gate": w_shared_gate, "w_shared_up": w_shared_up, "w_shared_down": w_shared_down, "w_dense_up": w_dense_up, "w_dense_down": w_dense_down, "dense_gate": dense_gate}


def norm_rows(values, gains):
    values = values.astype(jnp.float32)
    factor = lax.rsqrt(lax.optimization_barrier(jnp.mean(values * values, axis=-1, keepdims=True)) + 1e-06)
    return values * factor * gains.astype(jnp.float32)

def angles_at(positions, rot_width):
    half_width = rot_width // 2
    inverse = 1.0 / 10000.0 ** (jnp.arange(half_width, dtype=jnp.float32) / half_width)
    return positions.astype(jnp.float32)[..., None] * inverse

def rotate(values, angles):
    half_width = values.shape[-1] // 2
    first = values[..., :half_width]
    second = values[..., half_width:]
    cosines = jnp.cos(angles)
    sines = jnp.sin(angles)
    return jnp.concatenate([first * cosines - second * sines, first * sines + second * cosines], axis=-1)

def block_sum(act_values, down_weight):
    shares = jnp.einsum('rnf,nfd->rnd', act_values.astype(jnp.float32).reshape(act_values.shape[0], N_TP, -1), down_weight.astype(jnp.float32).reshape(N_TP, -1, MODEL_WIDTH))
    return lax.optimization_barrier(jnp.sum(lax.optimization_barrier(shares.astype(jnp.bfloat16)).astype(jnp.float32), axis=1))

def reference(hidden, lengths, latent_cache, cache_rotary, attn_gain, w_query_nope, w_query_rope, latent_weight, w_rotary_key, latent_norm_gain, key_up_weight, value_up_weight, head_gain, w_output, ffn_gain, expert_ids, expert_weights, w_expert_gate, w_expert_up, w_expert_down, w_shared_gate, w_shared_up, w_shared_down, w_dense_up, w_dense_down, dense_gate):
    normed = norm_rows(hidden, attn_gain).astype(jnp.bfloat16)
    query_unrotated = jnp.dot(normed, w_query_nope, preferred_element_type=jnp.float32).astype(jnp.bfloat16)
    query_unrotated = query_unrotated.reshape(SEQUENCE_COUNT, HEAD_COUNT, PLAIN_QUERY)
    query_rope = jnp.dot(normed, w_query_rope, preferred_element_type=jnp.float32).astype(jnp.bfloat16)
    query_rope = query_rope.reshape(SEQUENCE_COUNT, HEAD_COUNT, ROPE)
    query_in_latent = jnp.einsum('tba,bai->tbi', query_unrotated.astype(jnp.float32), key_up_weight.reshape(HEAD_COUNT, PLAIN_QUERY, LATENT_UNITS).astype(jnp.float32)).astype(jnp.bfloat16)
    angles = angles_at(lengths, ROPE)
    query_rotated = rotate(query_rope.astype(jnp.float32), angles[:, None, :]).astype(jnp.bfloat16)
    new_latent = norm_rows(jnp.dot(normed, latent_weight, preferred_element_type=jnp.float32), latent_norm_gain).astype(jnp.bfloat16)
    new_key = rotate(jnp.dot(normed, w_rotary_key, preferred_element_type=jnp.float32), angles).astype(jnp.bfloat16)
    score_scale = (PLAIN_QUERY + ROPE) ** (-0.5)

    def attend_one(inputs):
        latent_query_rows, rot_query, latents, rot_keys, seq_length, own_latent, own_key = inputs
        latent_query_rows = latent_query_rows.astype(jnp.float32)
        rot_query = rot_query.astype(jnp.float32)
        cache_scores = (jnp.dot(latent_query_rows, latents.astype(jnp.float32).T) + jnp.dot(rot_query, rot_keys.astype(jnp.float32))) * score_scale
        own_scores = (jnp.dot(latent_query_rows, own_latent.astype(jnp.float32)) + jnp.dot(rot_query, own_key.astype(jnp.float32))) * score_scale
        in_cache = jnp.arange(CACHE_LENGTH, dtype=jnp.int32) < seq_length
        cache_scores = jnp.where(in_cache[None, :], cache_scores, -jnp.inf)
        peak = jnp.maximum(lax.optimization_barrier(jnp.max(cache_scores, axis=-1)), own_scores)
        cache_exp = jnp.exp(cache_scores - peak[:, None])
        own_exp = jnp.exp(own_scores - peak)
        weight_sum = lax.optimization_barrier(jnp.sum(cache_exp, axis=-1)) + own_exp
        cache_probs = (cache_exp / weight_sum[:, None]).astype(jnp.bfloat16)
        own_probs = (own_exp / weight_sum).astype(jnp.bfloat16)
        mixed_output = jnp.dot(cache_probs.astype(jnp.float32), latents.astype(jnp.float32))
        mixed_output = mixed_output + own_probs.astype(jnp.float32)[:, None] * own_latent.astype(jnp.float32)[None, :]
        return mixed_output.astype(jnp.bfloat16)
    attended_value = lax.map(attend_one, (query_in_latent, query_rotated, latent_cache, cache_rotary, lengths, new_latent, new_key))
    head_output = jnp.einsum('bqc,cqp->bqp', attended_value.astype(jnp.float32), value_up_weight.reshape(LATENT_UNITS, HEAD_COUNT, VALUE_UNITS).astype(jnp.float32))
    head_output = norm_rows(head_output, head_gain.reshape(HEAD_COUNT, VALUE_UNITS)).astype(jnp.bfloat16).reshape(SEQUENCE_COUNT, HEAD_COUNT * VALUE_UNITS)
    attention = jnp.dot(head_output, w_output, preferred_element_type=jnp.float32)
    middle = (hidden.astype(jnp.float32) + attention).astype(jnp.bfloat16)
    normed_ffn = norm_rows(middle, ffn_gain).astype(jnp.bfloat16)
    group_ids = expert_ids.reshape(N_EP, SEQ_GRP * TOPK)
    matches = (group_ids[:, :, None] == jnp.arange(EXPERTS, dtype=jnp.int32)[None, None, :]).astype(jnp.int32)
    slot_index = lax.optimization_barrier(jnp.sum((jnp.cumsum(matches, axis=1) - matches) * matches, axis=2))
    target = (group_ids * CAP + slot_index).reshape(N_EP, SEQ_GRP, TOPK)
    places = jnp.arange(EXPERTS * CAP, dtype=jnp.int32)
    chosen = places[None, :, None, None] == target[:, None, :, :]
    dispatch = jnp.any(chosen, axis=3).astype(jnp.float32)
    grouped_rows = normed_ffn.reshape(N_EP, SEQ_GRP, MODEL_WIDTH).astype(jnp.float32)
    sent_rows = jnp.einsum('gcs,gsd->gcd', dispatch, grouped_rows).astype(jnp.bfloat16)
    sent_rows = jnp.swapaxes(sent_rows.reshape(N_EP, EXPERTS, CAP, MODEL_WIDTH), 0, 1).reshape(EXPERTS, N_EP * CAP, MODEL_WIDTH)

    def run_expert(inputs):
        expert_rows, gate_weight, up_weight, down_weight = inputs
        expert_rows = expert_rows.astype(jnp.float32)
        gate_pre = jnp.dot(expert_rows, gate_weight.astype(jnp.float32))
        up_pre = jnp.dot(expert_rows, up_weight.astype(jnp.float32))
        act_values = (jax.nn.silu(gate_pre) * up_pre).astype(jnp.bfloat16)
        return block_sum(act_values, down_weight).astype(jnp.bfloat16)
    slot_out = lax.map(run_expert, (sent_rows, w_expert_gate, w_expert_up, w_expert_down))
    slot_out = jnp.swapaxes(slot_out.reshape(EXPERTS, N_EP, CAP, MODEL_WIDTH), 0, 1).reshape(N_EP, EXPERTS * CAP, MODEL_WIDTH)
    group_weights = expert_weights.reshape(N_EP, SEQ_GRP, TOPK)
    combine = lax.optimization_barrier(jnp.sum(jnp.where(jnp.swapaxes(chosen, 1, 2), group_weights[:, :, None, :], 0.0), axis=3))
    routed = jnp.einsum('gsc,gcd->gsd', combine, slot_out.astype(jnp.float32), precision=lax.Precision.HIGHEST).reshape(SEQUENCE_COUNT, MODEL_WIDTH)
    shared_act = (jax.nn.silu(jnp.dot(normed_ffn, w_shared_gate, preferred_element_type=jnp.float32)) * jnp.dot(normed_ffn, w_shared_up, preferred_element_type=jnp.float32)).astype(jnp.bfloat16)
    dense_act = jax.nn.gelu(jnp.dot(normed_ffn, w_dense_up, preferred_element_type=jnp.float32)).astype(jnp.bfloat16)
    mix_gate = jax.nn.sigmoid(jnp.dot(normed_ffn, dense_gate, preferred_element_type=jnp.float32))
    shared_shares = jnp.einsum('rnf,nfd->rnd', shared_act.astype(jnp.float32).reshape(SEQUENCE_COUNT, N_TP, -1), w_shared_down.astype(jnp.float32).reshape(N_TP, -1, MODEL_WIDTH))
    dense_shares = jnp.einsum('rnf,nfd->rnd', dense_act.astype(jnp.float32).reshape(SEQUENCE_COUNT, N_TP, -1), w_dense_down.astype(jnp.float32).reshape(N_TP, -1, MODEL_WIDTH))
    side_terms = shared_shares + mix_gate[:, None, None] * dense_shares
    side = lax.optimization_barrier(jnp.sum(lax.optimization_barrier(side_terms.astype(jnp.bfloat16)).astype(jnp.float32), axis=1))
    return (middle.astype(jnp.float32) + routed + side).astype(jnp.bfloat16)
```

```python
import jax
import jax.numpy as jnp
from jax import lax
from jax.sharding import PartitionSpec as P

MODEL_WIDTH = 2048
PLAIN_QUERY = 64
ROPE = 32
LATENT_UNITS = 512
CAP = 2


def exchange(x, axis):
    return lax.all_to_all(x, axis, split_axis=0, concat_axis=0, tiled=True)


def column_tiles(x, peers):
    rows, cols = x.shape
    return jnp.swapaxes(x.reshape(rows, peers, cols // peers), 0, 1)


def norm_rows(values, gains):
    values = values.astype(jnp.float32)
    factor = lax.rsqrt(jnp.mean(values * values, axis=-1, keepdims=True) + 1e-06)
    return values * factor * gains.astype(jnp.float32)


def angles_at(positions, rot_width):
    half_width = rot_width // 2
    inverse = 1.0 / 10000.0 ** (jnp.arange(half_width, dtype=jnp.float32) / half_width)
    return positions.astype(jnp.float32)[..., None] * inverse


def rotate(values, angles):
    half_width = values.shape[-1] // 2
    first = values[..., :half_width]
    second = values[..., half_width:]
    cosines = jnp.cos(angles)
    sines = jnp.sin(angles)
    return jnp.concatenate(
        [first * cosines - second * sines, first * sines + second * cosines], axis=-1
    )


def three_parts(values):
    parts = []
    for _ in range(3):
        part = lax.reduce_precision(values, 8, 7)
        parts.append(part.astype(jnp.bfloat16))
        values = values - part
    return parts


def dot32(a, b):
    return jnp.dot(a, b, preferred_element_type=jnp.float32)


def on_device(
    hidden,
    lengths,
    latent_cache,
    cache_rotary,
    attn_gain,
    w_query_nope,
    w_query_rope,
    latent_weight,
    w_rotary_key,
    latent_norm_gain,
    key_up_weight,
    value_up_weight,
    head_gain,
    w_output,
    ffn_gain,
    expert_ids,
    expert_weights,
    w_expert_gate,
    w_expert_up,
    w_expert_down,
    w_shared_gate,
    w_shared_up,
    w_shared_down,
    w_dense_up,
    w_dense_down,
    dense_gate,
):
    tp = lax.axis_size("tp")
    ep = lax.axis_size("ep")
    tp_index = lax.axis_index("tp")
    rows = hidden.shape[0]
    cols = MODEL_WIDTH // tp

    flat_ids = expert_ids.reshape(-1)
    matches = (flat_ids[:, None] == jnp.arange(ep, dtype=jnp.int32)[None, :]).astype(jnp.int32)
    slot_index = jnp.sum((jnp.cumsum(matches, axis=0) - matches) * matches, axis=1)
    target = (flat_ids * CAP + slot_index).reshape(rows, -1)
    places = jnp.arange(ep * CAP, dtype=jnp.int32)
    chosen = places[:, None, None] == target[None, :, :]
    dispatch = jnp.any(chosen, axis=2).astype(jnp.bfloat16)
    combine = jnp.sum(jnp.where(chosen, expert_weights[None, :, :], 0.0), axis=2).T
    combine_parts = jnp.concatenate(three_parts(combine), axis=0)

    normed = norm_rows(hidden, attn_gain).astype(jnp.bfloat16)
    query_nope = dot32(normed, w_query_nope).astype(jnp.bfloat16)
    query_rope = dot32(normed, w_query_rope).astype(jnp.bfloat16)
    query_latent = dot32(query_nope, key_up_weight).astype(jnp.bfloat16)
    queries = exchange(jnp.concatenate([query_latent, query_rope], axis=1), "tp")

    own_row = lax.dynamic_slice_in_dim(normed, tp_index, 1, 0)
    angles = angles_at(lengths, ROPE)
    new_latent = norm_rows(dot32(own_row, latent_weight), latent_norm_gain).astype(jnp.bfloat16)
    new_key = rotate(dot32(own_row, w_rotary_key), angles).astype(jnp.bfloat16)

    query_rows = queries[:, :LATENT_UNITS]
    rot_query = rotate(queries[:, LATENT_UNITS:].astype(jnp.float32), angles).astype(jnp.bfloat16)
    latents = latent_cache[0]
    in_cache = jnp.arange(latents.shape[0], dtype=jnp.int32) < lengths[0]
    score_scale = (PLAIN_QUERY + ROPE) ** (-0.5)
    cache_scores = jnp.einsum("hr,lr->hl", query_rows, latents, preferred_element_type=jnp.float32)
    cache_scores = cache_scores + dot32(rot_query, cache_rotary[0])
    cache_scores = jnp.where(in_cache[None, :], cache_scores * score_scale, -jnp.inf)
    own_scores = jnp.sum(
        query_rows.astype(jnp.float32) * new_latent.astype(jnp.float32), axis=1
    ) + jnp.sum(rot_query.astype(jnp.float32) * new_key.astype(jnp.float32), axis=1)
    own_scores = own_scores * score_scale
    peak = jnp.maximum(jnp.max(cache_scores, axis=-1), own_scores)
    cache_exp = jnp.exp(cache_scores - peak[:, None])
    own_exp = jnp.exp(own_scores - peak)
    weight_sum = jnp.sum(cache_exp, axis=-1) + own_exp
    cache_probs = (cache_exp / weight_sum[:, None]).astype(jnp.bfloat16)
    own_probs = (own_exp / weight_sum).astype(jnp.bfloat16)
    attended = dot32(cache_probs, latents) + own_probs.astype(jnp.float32)[
        :, None
    ] * new_latent.astype(jnp.float32)
    attended = exchange(attended.astype(jnp.bfloat16), "tp")

    head_out = norm_rows(dot32(attended, value_up_weight), head_gain).astype(jnp.bfloat16)
    share = dot32(head_out, w_output).astype(jnp.bfloat16)
    attention = exchange(column_tiles(share, tp), "tp").astype(jnp.float32).sum(axis=0)
    own_hidden = lax.dynamic_slice_in_dim(hidden, tp_index * cols, cols, 1)
    own_middle = (own_hidden.astype(jnp.float32) + attention).astype(jnp.bfloat16)
    tiles = exchange(jnp.broadcast_to(own_middle[None], (tp, rows, cols)), "tp")
    middle = jnp.swapaxes(tiles, 0, 1).reshape(rows, MODEL_WIDTH)
    normed_ffn = norm_rows(middle, ffn_gain).astype(jnp.bfloat16)

    sent = dot32(dispatch, normed_ffn).astype(jnp.bfloat16).reshape(ep, CAP, MODEL_WIDTH)
    arrived = exchange(sent, "ep").reshape(ep * CAP, MODEL_WIDTH)
    expert_act = jax.nn.silu(dot32(arrived, w_expert_gate[0])) * dot32(arrived, w_expert_up[0])
    part = dot32(expert_act.astype(jnp.bfloat16), w_expert_down[0]).astype(jnp.bfloat16)
    returned = exchange(part.reshape(ep, CAP, MODEL_WIDTH), "ep").reshape(ep * CAP, MODEL_WIDTH)

    shared_act = (
        jax.nn.silu(dot32(normed_ffn, w_shared_gate)) * dot32(normed_ffn, w_shared_up)
    ).astype(jnp.bfloat16)
    dense_act = jax.nn.gelu(dot32(normed_ffn, w_dense_up)).astype(jnp.bfloat16)
    mix_gate = jax.nn.sigmoid(dot32(normed_ffn, dense_gate))
    side_part = dot32(shared_act, w_shared_down) + mix_gate[:, None] * dot32(
        dense_act, w_dense_down
    )

    routed_part = dot32(combine_parts, returned).reshape(3, rows, MODEL_WIDTH).sum(axis=0)
    total = (routed_part + side_part).astype(jnp.bfloat16)
    total = exchange(column_tiles(total, tp), "tp").astype(jnp.float32).sum(axis=0)
    return (own_middle.astype(jnp.float32) + total).astype(jnp.bfloat16)


def solution(mesh):
    placed = (
        P("ep", None),
        P(("ep", "tp")),
        P(("ep", "tp"), None, None),
        P(("ep", "tp"), None, None),
        P(),
        P(None, "tp"),
        P(None, "tp"),
        P(),
        P(),
        P(),
        P("tp", None),
        P(None, "tp"),
        P("tp"),
        P("tp", None),
        P(),
        P("ep", None),
        P("ep", None),
        P("ep", None, "tp"),
        P("ep", None, "tp"),
        P("ep", "tp", None),
        P(None, "tp"),
        P(None, "tp"),
        P("tp", None),
        P(None, "tp"),
        P("tp", None),
        P(),
    )
    return jax.shard_map(
        on_device, mesh=mesh, in_specs=placed, out_specs=P("ep", "tp"), check_vma=False
    )
```

```python
import jax
import jax.numpy as jnp
from jax import lax
from jax.experimental import pallas as pl
from jax.experimental.pallas import tpu as pltpu
from jax.sharding import PartitionSpec as P

MODEL_WIDTH = 2048
PLAIN_QUERY = 64
ROPE = 32
HALF = 16
LATENT_UNITS = 512
CAP = 2
LANES = 128
F32 = jnp.float32
BF16 = jnp.bfloat16
EPS = 1e-06


def exchange(x, axis):
    return lax.all_to_all(x, axis, split_axis=0, concat_axis=0, tiled=True)


def dot32(a, b):
    return jnp.dot(a, b, preferred_element_type=F32)


def dot_t(a, b):
    return lax.dot_general(a, b, (((1,), (1,)), ((), ())), preferred_element_type=F32)


def call(body, outs, args, smem=(), scratch=()):
    vmem = pl.BlockSpec(memory_space=pltpu.VMEM)
    in_specs = [
        pl.BlockSpec(memory_space=pltpu.SMEM) if i in smem else vmem for i in range(len(args))
    ]
    return pl.pallas_call(
        body,
        out_shape=outs,
        in_specs=in_specs,
        out_specs=jax.tree.map(lambda _: vmem, outs),
        scratch_shapes=list(scratch),
    )(*args)


def shape(dims, dtype):
    return jax.ShapeDtypeStruct(dims, dtype)


def query_body(hidden, gain, w_nope, w_rope, key_up, out, normed_out):
    values = hidden[...].astype(F32)
    factor = lax.rsqrt(jnp.mean(values * values, axis=-1, keepdims=True) + EPS)
    normed = (values * factor * gain[...]).astype(BF16)
    normed_out[...] = normed
    nope = dot_t(normed, w_nope[...]).astype(BF16)
    rope = dot_t(normed, w_rope[...]).astype(BF16).astype(F32)
    latent = dot32(nope, key_up[...]).astype(BF16).astype(F32)
    for s in range(LATENT_UNITS // LANES):
        out[:, s, :] = latent[:, s * LANES : (s + 1) * LANES]
    rows = out.shape[0]
    out[:, 4, :] = jnp.concatenate([rope, jnp.zeros((rows, LANES - ROPE), F32)], axis=1)
    for s in range(5, 8):
        out[:, s, :] = jnp.zeros((rows, LANES), F32)


def rotated(values, cos, sin):
    first, second = values[:, :HALF], values[:, HALF:ROPE]
    return jnp.concatenate([first * cos - second * sin, first * sin + second * cos], axis=1)


def new_token_body(index, normed, w_latent, w_key, gain, cos, sin, latent_out, key_out):
    latent = dot32(normed[...], w_latent[...])
    key = dot_t(normed[...], w_key[...])
    rows = lax.broadcasted_iota(jnp.int32, (latent.shape[0], 1), 0)
    mine = rows == index[0]
    latent = jnp.sum(jnp.where(mine, latent, 0.0), axis=0, keepdims=True)
    key = jnp.sum(jnp.where(mine, key, 0.0), axis=0, keepdims=True)
    factor = lax.rsqrt(jnp.mean(latent * latent, axis=-1, keepdims=True) + EPS)
    latent_out[...] = (latent * factor * gain[...]).astype(BF16).astype(F32)
    key_out[...] = rotated(key, cos[...], sin[...]).astype(BF16).astype(F32)


def attention_body(lengths, queries, latents, rotary, new_latent, new_key, cos, sin, out):
    parts = [queries[:, s, :] for s in range(LATENT_UNITS // LANES)]
    query = jnp.concatenate(parts, axis=1)
    rope = rotated(queries[:, 4, :], cos[...], sin[...]).astype(BF16)
    scale = (PLAIN_QUERY + ROPE) ** (-0.5)
    cache = latents[0]
    scores = dot_t(query.astype(BF16), cache) + dot32(rope, rotary[0])
    place = lax.broadcasted_iota(jnp.int32, scores.shape, 1)
    scores = jnp.where(place < lengths[0], scores * scale, -jnp.inf)
    own = jnp.sum(query * new_latent[...], axis=1, keepdims=True)
    own = own + jnp.sum(rope.astype(F32) * new_key[...], axis=1, keepdims=True)
    own = own * scale
    peak = jnp.maximum(jnp.max(scores, axis=1, keepdims=True), own)
    cache_exp = jnp.exp(scores - peak)
    own_exp = jnp.exp(own - peak)
    total = jnp.sum(cache_exp, axis=1, keepdims=True) + own_exp
    probs = (cache_exp / total).astype(BF16)
    own_probs = (own_exp / total).astype(BF16).astype(F32)
    mixed = dot32(probs, cache) + own_probs * new_latent[...]
    mixed = mixed.astype(BF16).astype(F32)
    for s in range(LATENT_UNITS // LANES):
        out[:, s, :] = mixed[:, s * LANES : (s + 1) * LANES]
    for s in range(4, 8):
        out[:, s, :] = jnp.zeros((out.shape[0], LANES), F32)


def head_body(attended, value_up, gain, w_output, out):
    parts = [attended[:, s, :] for s in range(LATENT_UNITS // LANES)]
    values = jnp.concatenate(parts, axis=1).astype(BF16)
    head = dot_t(values, value_up[...])
    factor = lax.rsqrt(jnp.mean(head * head, axis=-1, keepdims=True) + EPS)
    head = (head * factor * gain[...]).astype(BF16)
    share = dot32(head, w_output[...]).astype(BF16)
    for j in range(out.shape[0]):
        out[j] = share[:, j * LANES : (j + 1) * LANES]


def middle_body(index, shares, hidden, out):
    total = shares[0].astype(F32)
    for j in range(1, shares.shape[0]):
        total = total + shares[j].astype(F32)
    start = pl.multiple_of(index[0] * LANES, LANES)
    middle = (hidden[:, pl.ds(start, LANES)].astype(F32) + total).astype(BF16)
    for j in range(out.shape[0]):
        out[j] = middle


def dispatch_body(tiles, gain, dispatch, normed_out, out, wide):
    count = tiles.shape[0]
    values = [tiles[j].astype(F32) for j in range(count)]
    square = values[0] * values[0]
    for j in range(1, count):
        square = square + values[j] * values[j]
    mean = jnp.sum(square, axis=1, keepdims=True) * (1.0 / MODEL_WIDTH)
    factor = lax.rsqrt(mean + EPS)
    slots = dispatch.shape[0]
    for j in range(count):
        tile = slice(j * LANES, (j + 1) * LANES)
        normed = (values[j] * factor * gain[:, tile]).astype(BF16)
        normed_out[:, tile] = normed
        wide[pl.ds(j, slots, stride=count), :] = dot32(dispatch[...], normed)
    rows = slots * count // out.shape[0]
    for p in range(out.shape[0]):
        out[p] = wide[p * rows : (p + 1) * rows, :].astype(BF16)


def side_body(normed, w_gate, w_up, w_shared_down, w_dense_up, w_dense_down, gate, out):
    x = normed[...]
    pre = dot_t(x, w_gate[...])
    shared = (pre / (1.0 + jnp.exp(-pre)) * dot_t(x, w_up[...])).astype(BF16)
    dense = jax.nn.gelu(dot32(x, w_dense_up[...])).astype(BF16)
    logit = jnp.sum(x.astype(F32) * gate[...], axis=1, keepdims=True)
    mix = 1.0 / (1.0 + jnp.exp(-logit))
    out[...] = dot32(shared, w_shared_down[...]) + mix * dot32(dense, w_dense_down[...])


def expert_body(arrived, w_gate, w_up, w_down, out, wide, rows_in):
    peers, rows, _ = arrived.shape
    count = MODEL_WIDTH // LANES
    slots = peers * rows // count
    for p in range(peers):
        wide[p * rows : (p + 1) * rows, :] = arrived[p].astype(F32)
    for j in range(count):
        tile = slice(j * LANES, (j + 1) * LANES)
        rows_in[:, tile] = wide[pl.ds(j, slots, stride=count), :].astype(BF16)
    x = rows_in[...]
    pre = dot32(x, w_gate[0])
    act = (pre / (1.0 + jnp.exp(-pre)) * dot32(x, w_up[0])).astype(BF16)
    part = dot32(act, w_down[0])
    for j in range(count):
        wide[pl.ds(j, slots, stride=count), :] = part[:, j * LANES : (j + 1) * LANES]
    for p in range(peers):
        out[p] = wide[p * rows : (p + 1) * rows, :].astype(BF16)


def combine_body(returned, weights, side, out, wide):
    peers, rows, _ = returned.shape
    count = MODEL_WIDTH // LANES
    slots = peers * rows // count
    tokens = side.shape[0]
    for p in range(peers):
        wide[p * rows : (p + 1) * rows, :] = returned[p].astype(F32)
    for j in range(count):
        block = wide[pl.ds(j, slots, stride=count), :].astype(BF16)
        sums = dot32(weights[...], block)
        routed = sums[:tokens] + sums[tokens : 2 * tokens] + sums[2 * tokens :]
        out[j] = (routed + side[:, j * LANES : (j + 1) * LANES]).astype(BF16)


def final_body(tiles, middle, out):
    total = tiles[0].astype(F32)
    for j in range(1, tiles.shape[0]):
        total = total + tiles[j].astype(F32)
    out[...] = (middle[0].astype(F32) + total).astype(BF16)


def three_parts(values):
    parts = []
    for _ in range(3):
        part = lax.reduce_precision(values, 8, 7)
        parts.append(part.astype(BF16))
        values = values - part
    return jnp.concatenate(parts, axis=0)


def row(gain):
    return gain.astype(F32)[None, :]


def on_device(
    hidden,
    lengths,
    latent_cache,
    cache_rotary,
    attn_gain,
    w_query_nope,
    w_query_rope,
    latent_weight,
    w_rotary_key,
    latent_norm_gain,
    key_up_weight,
    value_up_weight,
    head_gain,
    w_output,
    ffn_gain,
    expert_ids,
    expert_weights,
    w_expert_gate,
    w_expert_up,
    w_expert_down,
    w_shared_gate,
    w_shared_up,
    w_shared_down,
    w_dense_up,
    w_dense_down,
    dense_gate,
):
    tp = lax.axis_size("tp")
    ep = lax.axis_size("ep")
    index = lax.axis_index("tp").astype(jnp.int32).reshape(1)
    rows = hidden.shape[0]
    slots = ep * CAP
    small = shape((tp, 8, LANES), F32)
    tiles = shape((tp, rows, LANES), BF16)
    routed_rows = slots * tp // ep
    large = shape((ep, routed_rows, LANES), BF16)
    wide = pltpu.VMEM((slots * tp, LANES), F32)

    payload, normed = call(
        query_body,
        (small, shape(hidden.shape, BF16)),
        (hidden, row(attn_gain), w_query_nope.T, w_query_rope.T, key_up_weight),
    )
    queries = exchange(payload, "tp")

    inverse = 1.0 / 10000.0 ** (jnp.arange(HALF, dtype=F32) / HALF)
    angles = lengths.astype(F32)[:, None] * inverse[None, :]
    cos, sin = jnp.cos(angles), jnp.sin(angles)
    new_latent, new_key = call(
        new_token_body,
        (shape((1, LATENT_UNITS), F32), shape((1, ROPE), F32)),
        (index, normed, latent_weight, w_rotary_key.T, row(latent_norm_gain), cos, sin),
        smem=(0,),
    )

    flat_ids = expert_ids.reshape(-1)
    matches = (flat_ids[:, None] == jnp.arange(ep, dtype=jnp.int32)[None, :]).astype(jnp.int32)
    slot_index = jnp.sum((jnp.cumsum(matches, axis=0) - matches) * matches, axis=1)
    target = (flat_ids * CAP + slot_index).reshape(rows, -1)
    places = jnp.arange(slots, dtype=jnp.int32)
    chosen = places[:, None, None] == target[None, :, :]
    dispatch = jnp.any(chosen, axis=2).astype(BF16)
    combine = three_parts(jnp.sum(jnp.where(chosen, expert_weights[None, :, :], 0.0), axis=2).T)

    payload = call(
        attention_body,
        small,
        (lengths, queries, latent_cache, cache_rotary, new_latent, new_key, cos, sin),
        smem=(0,),
    )
    attended = exchange(payload, "tp")

    payload = call(head_body, tiles, (attended, value_up_weight.T, row(head_gain), w_output))
    shares = exchange(payload, "tp")
    own_middle = call(middle_body, tiles, (index, shares, hidden), smem=(0,))
    middle = exchange(own_middle, "tp")

    normed_ffn, payload = call(
        dispatch_body,
        (shape(hidden.shape, BF16), large),
        (middle, row(ffn_gain), dispatch),
        scratch=(wide,),
    )
    arrived = exchange(payload, "ep")
    side = call(
        side_body,
        shape(hidden.shape, F32),
        (
            normed_ffn,
            w_shared_gate.T,
            w_shared_up.T,
            w_shared_down,
            w_dense_up,
            w_dense_down,
            row(dense_gate),
        ),
    )
    payload = call(
        expert_body,
        large,
        (arrived, w_expert_gate, w_expert_up, w_expert_down),
        scratch=(wide, pltpu.VMEM((slots, MODEL_WIDTH), BF16)),
    )
    returned = exchange(payload, "ep")

    payload = call(combine_body, tiles, (returned, combine, side), scratch=(wide,))
    parts = exchange(payload, "tp")
    return call(final_body, shape((rows, LANES), BF16), (parts, own_middle))


def solution(mesh):
    placed = (
        P("ep", None),
        P(("ep", "tp")),
        P(("ep", "tp"), None, None),
        P(("ep", "tp"), None, None),
        P(),
        P(None, "tp"),
        P(None, "tp"),
        P(),
        P(),
        P(),
        P("tp", None),
        P(None, "tp"),
        P("tp"),
        P("tp", None),
        P(),
        P("ep", None),
        P("ep", None),
        P("ep", None, "tp"),
        P("ep", None, "tp"),
        P("ep", "tp", None),
        P(None, "tp"),
        P(None, "tp"),
        P("tp", None),
        P(None, "tp"),
        P("tp", None),
        P(),
    )
    return jax.shard_map(
        on_device, mesh=mesh, in_specs=placed, out_specs=P("ep", "tp"), check_vma=False
    )
```

```python
import jax
import jax.numpy as jnp
from jax import lax
from jax.experimental import pallas as pl
from jax.experimental.pallas import tpu as pltpu
from jax.sharding import PartitionSpec as P

MODEL_WIDTH = 2048
PLAIN_QUERY = 64
ROPE = 32
HALF = 16
LATENT_UNITS = 512
CAP = 2
LANES = 128
F32 = jnp.float32
BF16 = jnp.bfloat16
EPS = 1e-06


def exchange(x, axis):
    return lax.all_to_all(x, axis, split_axis=0, concat_axis=0, tiled=True)


def dot32(a, b):
    return jnp.dot(a, b, preferred_element_type=F32)


def dot_t(a, b):
    return lax.dot_general(a, b, (((1,), (1,)), ((), ())), preferred_element_type=F32)


def call(body, outs, args, smem=(), hbm=(), raw=(), scratch=(), leave=False):
    vmem = pl.BlockSpec(memory_space=pltpu.VMEM)
    kinds = {i: pl.BlockSpec(memory_space=pltpu.SMEM) for i in smem}
    kinds.update({i: pl.BlockSpec(memory_space=pl.ANY) for i in raw})
    free = set(smem) | set(hbm) | set(raw)
    args = [
        x if i in free else pltpu.with_memory_space_constraint(x, pltpu.VMEM)
        for i, x in enumerate(args)
    ]
    place = (lambda o: o) if leave else (lambda o: pltpu.VMEM(o.shape, o.dtype))
    return pl.pallas_call(
        body,
        out_shape=jax.tree.map(place, outs),
        in_specs=[kinds.get(i, vmem) for i in range(len(args))],
        out_specs=jax.tree.map(lambda _: vmem, outs),
        scratch_shapes=list(scratch),
    )(*args)


def together(*values):
    return lax.optimization_barrier(values)


def shape(dims, dtype):
    return jax.ShapeDtypeStruct(dims, dtype)


def row(gain):
    return gain[...].astype(F32).reshape(1, -1)


def query_body(hidden, gain, w_nope, w_rope, key_up, out, normed_out):
    values = hidden[...].astype(F32)
    factor = lax.rsqrt(jnp.mean(values * values, axis=-1, keepdims=True) + EPS)
    normed = (values * factor * row(gain)).astype(BF16)
    normed_out[...] = normed
    nope = dot_t(normed, w_nope[...]).astype(BF16)
    rope = dot_t(normed, w_rope[...]).astype(BF16).astype(F32)
    latent = dot32(nope, key_up[...]).astype(BF16).astype(F32)
    for s in range(LATENT_UNITS // LANES):
        out[:, s, :] = latent[:, s * LANES : (s + 1) * LANES]
    rows = out.shape[0]
    out[:, 4, :] = jnp.concatenate([rope, jnp.zeros((rows, LANES - ROPE), F32)], axis=1)
    for s in range(5, 8):
        out[:, s, :] = jnp.zeros((rows, LANES), F32)


def rotated(values, cos, sin):
    first, second = values[:, :HALF], values[:, HALF:ROPE]
    return jnp.concatenate([first * cos - second * sin, first * sin + second * cos], axis=1)


def new_token_body(
    index, normed, w_latent, w_key, gain, cos, sin, cache, rotary, latent_out, key_out, cache_out, rotary_out, sems
):
    copies = [
        pltpu.make_async_copy(cache, cache_out, sems.at[0]),
        pltpu.make_async_copy(rotary, rotary_out, sems.at[1]),
    ]
    for copy in copies:
        copy.start()
    latent = dot32(normed[...], w_latent[...])
    key = dot_t(normed[...], w_key[...])
    rows = lax.broadcasted_iota(jnp.int32, (latent.shape[0], 1), 0)
    mine = rows == index[0]
    latent = jnp.sum(jnp.where(mine, latent, 0.0), axis=0, keepdims=True)
    key = jnp.sum(jnp.where(mine, key, 0.0), axis=0, keepdims=True)
    factor = lax.rsqrt(jnp.mean(latent * latent, axis=-1, keepdims=True) + EPS)
    latent_out[...] = (latent * factor * row(gain)).astype(BF16).astype(F32)
    key_out[...] = rotated(key, cos[...], sin[...]).astype(BF16).astype(F32)
    for copy in copies:
        copy.wait()


def attention_body(lengths, queries, latents, rotary, new_latent, new_key, cos, sin, out):
    parts = [queries[:, s, :] for s in range(LATENT_UNITS // LANES)]
    query = jnp.concatenate(parts, axis=1)
    rope = rotated(queries[:, 4, :], cos[...], sin[...]).astype(BF16)
    scale = (PLAIN_QUERY + ROPE) ** (-0.5)
    cache = latents[0]
    scores = dot_t(query.astype(BF16), cache) + dot32(rope, rotary[0])
    place = lax.broadcasted_iota(jnp.int32, scores.shape, 1)
    scores = jnp.where(place < lengths[0], scores * scale, -jnp.inf)
    own = jnp.sum(query * new_latent[...], axis=1, keepdims=True)
    own = own + jnp.sum(rope.astype(F32) * new_key[...], axis=1, keepdims=True)
    own = own * scale
    peak = jnp.maximum(jnp.max(scores, axis=1, keepdims=True), own)
    cache_exp = jnp.exp(scores - peak)
    own_exp = jnp.exp(own - peak)
    total = jnp.sum(cache_exp, axis=1, keepdims=True) + own_exp
    probs = (cache_exp / total).astype(BF16)
    own_probs = (own_exp / total).astype(BF16).astype(F32)
    mixed = dot32(probs, cache) + own_probs * new_latent[...]
    mixed = mixed.astype(BF16).astype(F32)
    for s in range(LATENT_UNITS // LANES):
        out[:, s, :] = mixed[:, s * LANES : (s + 1) * LANES]
    for s in range(4, 8):
        out[:, s, :] = jnp.zeros((out.shape[0], LANES), F32)


def head_body(attended, value_up, gain, w_output, out):
    parts = [attended[:, s, :] for s in range(LATENT_UNITS // LANES)]
    values = jnp.concatenate(parts, axis=1).astype(BF16)
    head = dot_t(values, value_up[...])
    factor = lax.rsqrt(jnp.mean(head * head, axis=-1, keepdims=True) + EPS)
    head = (head * factor * row(gain)).astype(BF16)
    share = dot32(head, w_output[...]).astype(BF16)
    for j in range(out.shape[0]):
        out[j] = share[:, j * LANES : (j + 1) * LANES]


def middle_body(index, shares, hidden, out):
    total = shares[0].astype(F32)
    for j in range(1, shares.shape[0]):
        total = total + shares[j].astype(F32)
    start = pl.multiple_of(index[0] * LANES, LANES)
    middle = (hidden[:, pl.ds(start, LANES)].astype(F32) + total).astype(BF16)
    for j in range(out.shape[0]):
        out[j] = middle


def dispatch_body(tiles, gain, dispatch, normed_out, out, wide):
    count = tiles.shape[0]
    values = [tiles[j].astype(F32) for j in range(count)]
    square = values[0] * values[0]
    for j in range(1, count):
        square = square + values[j] * values[j]
    mean = jnp.sum(square, axis=1, keepdims=True) * (1.0 / MODEL_WIDTH)
    factor = lax.rsqrt(mean + EPS)
    slots = dispatch.shape[0]
    gains = row(gain)
    for j in range(count):
        tile = slice(j * LANES, (j + 1) * LANES)
        normed = (values[j] * factor * gains[:, tile]).astype(BF16)
        normed_out[:, tile] = normed
        wide[pl.ds(j, slots, stride=count), :] = dot32(dispatch[...], normed)
    rows = slots * count // out.shape[0]
    for p in range(out.shape[0]):
        out[p] = wide[p * rows : (p + 1) * rows, :].astype(BF16)


def side_body(normed, w_gate, w_up, w_shared_down, w_dense_up, w_dense_down, gate, out):
    x = normed[...]
    pre = dot_t(x, w_gate[...])
    shared = (pre / (1.0 + jnp.exp(-pre)) * dot_t(x, w_up[...])).astype(BF16)
    dense = jax.nn.gelu(dot32(x, w_dense_up[...])).astype(BF16)
    logit = jnp.sum(x.astype(F32) * row(gate), axis=1, keepdims=True)
    mix = 1.0 / (1.0 + jnp.exp(-logit))
    out[...] = dot32(shared, w_shared_down[...]) + mix * dot32(dense, w_dense_down[...])


def expert_body(arrived, w_gate, w_up, w_down, out, wide, rows_in):
    peers, rows, _ = arrived.shape
    count = MODEL_WIDTH // LANES
    slots = peers * rows // count
    for p in range(peers):
        wide[p * rows : (p + 1) * rows, :] = arrived[p].astype(F32)
    for j in range(count):
        tile = slice(j * LANES, (j + 1) * LANES)
        rows_in[:, tile] = wide[pl.ds(j, slots, stride=count), :].astype(BF16)
    x = rows_in[...]
    pre = dot32(x, w_gate[0])
    act = (pre / (1.0 + jnp.exp(-pre)) * dot32(x, w_up[0])).astype(BF16)
    part = dot32(act, w_down[0])
    for j in range(count):
        wide[pl.ds(j, slots, stride=count), :] = part[:, j * LANES : (j + 1) * LANES]
    for p in range(peers):
        out[p] = wide[p * rows : (p + 1) * rows, :].astype(BF16)


def combine_body(returned, weights, side, out, wide):
    peers, rows, _ = returned.shape
    count = MODEL_WIDTH // LANES
    slots = peers * rows // count
    tokens = side.shape[0]
    for p in range(peers):
        wide[p * rows : (p + 1) * rows, :] = returned[p].astype(F32)
    for j in range(count):
        block = wide[pl.ds(j, slots, stride=count), :].astype(BF16)
        sums = dot32(weights[...], block)
        routed = sums[:tokens] + sums[tokens : 2 * tokens] + sums[2 * tokens :]
        out[j] = (routed + side[:, j * LANES : (j + 1) * LANES]).astype(BF16)


def final_body(tiles, middle, out):
    total = tiles[0].astype(F32)
    for j in range(1, tiles.shape[0]):
        total = total + tiles[j].astype(F32)
    out[...] = (middle[0].astype(F32) + total).astype(BF16)


def three_parts(values):
    parts = []
    for _ in range(3):
        part = lax.reduce_precision(values, 8, 7)
        parts.append(part.astype(BF16))
        values = values - part
    return jnp.concatenate(parts, axis=0)


def on_device(
    hidden,
    lengths,
    latent_cache,
    cache_rotary,
    attn_gain,
    w_query_nope,
    w_query_rope,
    latent_weight,
    w_rotary_key,
    latent_norm_gain,
    key_up_weight,
    value_up_weight,
    head_gain,
    w_output,
    ffn_gain,
    expert_ids,
    expert_weights,
    w_expert_gate,
    w_expert_up,
    w_expert_down,
    w_shared_gate,
    w_shared_up,
    w_shared_down,
    w_dense_up,
    w_dense_down,
    dense_gate,
):
    tp = lax.axis_size("tp")
    ep = lax.axis_size("ep")
    index = lax.axis_index("tp").astype(jnp.int32).reshape(1)
    rows = hidden.shape[0]
    slots = ep * CAP
    small = shape((tp, 8, LANES), F32)
    tiles = shape((tp, rows, LANES), BF16)
    routed_rows = slots * tp // ep
    large = shape((ep, routed_rows, LANES), BF16)
    wide = pltpu.VMEM((slots * tp, LANES), F32)

    payload, normed = call(
        query_body,
        (small, shape(hidden.shape, BF16)),
        (hidden, attn_gain, w_query_nope.T, w_query_rope.T, key_up_weight),
        hbm=range(5),
    )
    queries = exchange(payload, "tp")

    inverse = 1.0 / 10000.0 ** (jnp.arange(HALF, dtype=F32) / HALF)
    angles = lengths.astype(F32)[:, None] * inverse[None, :]
    cos, sin = jnp.cos(angles), jnp.sin(angles)
    new_latent, new_key, cache, rotary = call(
        new_token_body,
        (
            shape((1, LATENT_UNITS), F32),
            shape((1, ROPE), F32),
            shape(latent_cache.shape, BF16),
            shape(cache_rotary.shape, BF16),
        ),
        (
            index,
            normed,
            latent_weight,
            w_rotary_key.T,
            latent_norm_gain,
            cos,
            sin,
            latent_cache,
            cache_rotary,
        ),
        smem=(0,),
        hbm=(2, 3, 4, 5, 6),
        raw=(7, 8),
        scratch=(pltpu.SemaphoreType.DMA((2,)),),
    )
    flat_ids = expert_ids.reshape(-1)
    matches = (flat_ids[:, None] == jnp.arange(ep, dtype=jnp.int32)[None, :]).astype(jnp.int32)
    slot_index = jnp.sum((jnp.cumsum(matches, axis=0) - matches) * matches, axis=1)
    target = (flat_ids * CAP + slot_index).reshape(rows, -1)
    places = jnp.arange(slots, dtype=jnp.int32)
    chosen = places[:, None, None] == target[None, :, :]
    dispatch = jnp.any(chosen, axis=2).astype(BF16)
    queries, new_latent, new_key, dispatch = together(queries, new_latent, new_key, dispatch)

    payload = call(
        attention_body,
        small,
        (lengths, queries, cache, rotary, new_latent, new_key, cos, sin),
        smem=(0,),
    )
    attended = exchange(payload, "tp")

    payload = call(head_body, tiles, (attended, value_up_weight.T, head_gain, w_output))
    shares = exchange(payload, "tp")
    own_middle = call(middle_body, tiles, (index, shares, hidden), smem=(0,))
    middle = exchange(own_middle, "tp")

    normed_ffn, payload = call(
        dispatch_body,
        (shape(hidden.shape, BF16), large),
        (middle, ffn_gain, dispatch),
        scratch=(wide,),
    )
    arrived = exchange(payload, "ep")
    side = call(
        side_body,
        shape(hidden.shape, F32),
        (
            normed_ffn,
            w_shared_gate.T,
            w_shared_up.T,
            w_shared_down,
            w_dense_up,
            w_dense_down,
            dense_gate,
        ),
        hbm=range(1, 7),
    )
    combine = three_parts(jnp.sum(jnp.where(chosen, expert_weights[None, :, :], 0.0), axis=2).T)
    arrived, side, combine = together(arrived, side, combine)
    payload = call(
        expert_body,
        large,
        (arrived, w_expert_gate, w_expert_up, w_expert_down),
        scratch=(wide, pltpu.VMEM((slots, MODEL_WIDTH), BF16)),
    )
    returned = exchange(payload, "ep")

    payload = call(combine_body, tiles, (returned, combine, side), scratch=(wide,))
    parts = exchange(payload, "tp")
    return call(final_body, shape((rows, LANES), BF16), (parts, own_middle), leave=True)


def solution(mesh):
    placed = (
        P("ep", None),
        P(("ep", "tp")),
        P(("ep", "tp"), None, None),
        P(("ep", "tp"), None, None),
        P(),
        P(None, "tp"),
        P(None, "tp"),
        P(),
        P(),
        P(),
        P("tp", None),
        P(None, "tp"),
        P("tp"),
        P("tp", None),
        P(),
        P("ep", None),
        P("ep", None),
        P("ep", None, "tp"),
        P("ep", None, "tp"),
        P("ep", "tp", None),
        P(None, "tp"),
        P(None, "tp"),
        P("tp", None),
        P(None, "tp"),
        P("tp", None),
        P(),
    )
    return jax.shard_map(
        on_device, mesh=mesh, in_specs=placed, out_specs=P("ep", "tp"), check_vma=False
    )
```

```python
import jax
import jax.numpy as jnp
from jax import lax
from jax.experimental import pallas as pl
from jax.experimental.pallas import tpu as pltpu
from jax.sharding import PartitionSpec as P

MODEL_WIDTH = 2048
PLAIN_QUERY = 64
ROPE = 32
HALF = 16
LATENT_UNITS = 512
CAP = 2
LANES = 128
F32 = jnp.float32
BF16 = jnp.bfloat16
EPS = 1e-06


def exchange(x, axis, groups=None):
    return lax.all_to_all(
        x, axis, split_axis=0, concat_axis=0, axis_index_groups=groups, tiled=True
    )


def core_swap(x):
    return lax.ppermute(x, "tp", [(i, i ^ 1) for i in range(lax.axis_size("tp"))])


def dot32(a, b):
    return jnp.dot(a, b, preferred_element_type=F32)


def dot_t(a, b):
    return lax.dot_general(a, b, (((1,), (1,)), ((), ())), preferred_element_type=F32)


def call(body, outs, args, smem=(), hbm=(), raw=(), scratch=(), leave=()):
    vmem = pl.BlockSpec(memory_space=pltpu.VMEM)
    kinds = {i: pl.BlockSpec(memory_space=pltpu.SMEM) for i in smem}
    kinds.update({i: pl.BlockSpec(memory_space=pl.ANY) for i in raw})
    free = set(smem) | set(hbm) | set(raw)
    scalars = set(smem)
    args = [
        x
        if i in scalars
        else pltpu.with_memory_space_constraint(x, pltpu.HBM if i in free else pltpu.VMEM)
        for i, x in enumerate(args)
    ]
    leaves, tree = jax.tree.flatten(outs)
    outs = tree.unflatten(
        (pltpu.HBM if i in leave else pltpu.VMEM)(o.shape, o.dtype) for i, o in enumerate(leaves)
    )
    return pl.pallas_call(
        body,
        out_shape=outs,
        in_specs=[kinds.get(i, vmem) for i in range(len(args))],
        out_specs=tree.unflatten(vmem for _ in leaves),
        scratch_shapes=list(scratch),
        compiler_params=pltpu.CompilerParams(vmem_limit_bytes=16 * 1024 * 1024),
    )(*args)


def together(*values):
    return lax.optimization_barrier(values)


def shape(dims, dtype):
    return jax.ShapeDtypeStruct(dims, dtype)


def row(gain):
    return gain[...].astype(F32).reshape(1, -1)


def query_body(hidden, gain, w_nope, w_rope, key_up, out, normed_out):
    values = hidden[...].astype(F32)
    factor = lax.rsqrt(jnp.mean(values * values, axis=-1, keepdims=True) + EPS)
    normed = (values * factor * row(gain)).astype(BF16)
    normed_out[...] = normed
    nope = dot_t(normed, w_nope[...]).astype(BF16)
    rope = dot_t(normed, w_rope[...]).astype(BF16).astype(F32)
    latent = dot32(nope, key_up[...]).astype(BF16).astype(F32)
    for s in range(LATENT_UNITS // LANES):
        out[:, s, :] = latent[:, s * LANES : (s + 1) * LANES]
    rows = out.shape[0]
    out[:, 4, :] = jnp.concatenate([rope, jnp.zeros((rows, LANES - ROPE), F32)], axis=1)
    for s in range(5, 8):
        out[:, s, :] = jnp.zeros((rows, LANES), F32)


def rotated(values, cos, sin):
    first, second = values[:, :HALF], values[:, HALF:ROPE]
    return jnp.concatenate([first * cos - second * sin, first * sin + second * cos], axis=1)


def new_token_body(
    index, normed, w_latent, w_key, gain, cos, sin, cache, rotary, out, cache_out, sems
):
    places, width = cache.shape[1:]
    copies = [pltpu.make_async_copy(cache.at[0], cache_out.at[pl.ds(0, places)], sems.at[0])]
    for k in range(rotary.shape[2] // width):
        source = rotary.at[0, :, pl.ds(k * width, width)]
        target = cache_out.at[pl.ds(places + k * ROPE, ROPE)]
        copies.append(pltpu.make_async_copy(source, target, sems.at[k + 1]))
    for copy in copies:
        copy.start()
    latent = dot32(normed[...], w_latent[...])
    key = dot_t(normed[...], w_key[...])
    rows = lax.broadcasted_iota(jnp.int32, (latent.shape[0], 1), 0)
    mine = rows == index[0]
    latent = jnp.sum(jnp.where(mine, latent, 0.0), axis=0, keepdims=True)
    key = jnp.sum(jnp.where(mine, key, 0.0), axis=0, keepdims=True)
    factor = lax.rsqrt(jnp.mean(latent * latent, axis=-1, keepdims=True) + EPS)
    out[:, :LATENT_UNITS] = (latent * factor * row(gain)).astype(BF16).astype(F32)
    key = rotated(key, cos[...], sin[...]).astype(BF16).astype(F32)
    out[:, LATENT_UNITS:] = jnp.concatenate([key, jnp.zeros((1, LANES - ROPE), F32)], axis=1)
    for copy in copies:
        copy.wait()


def attention_body(lengths, queries, caches, token, cos, sin, out):
    new_latent = token[:, :LATENT_UNITS]
    new_key = token[:, LATENT_UNITS : LATENT_UNITS + ROPE]
    parts = [queries[:, s, :] for s in range(LATENT_UNITS // LANES)]
    query = jnp.concatenate(parts, axis=1)
    rope = rotated(queries[:, 4, :], cos[...], sin[...]).astype(BF16)
    scale = (PLAIN_QUERY + ROPE) ** (-0.5)
    count = caches.shape[0] * LATENT_UNITS // (LATENT_UNITS + ROPE)
    cache = caches[:count, :]
    turned = [
        dot32(rope, caches[count + k * ROPE : count + (k + 1) * ROPE, :])
        for k in range(count // LATENT_UNITS)
    ]
    scores = dot_t(query.astype(BF16), cache) + jnp.concatenate(turned, axis=1)
    place = lax.broadcasted_iota(jnp.int32, scores.shape, 1)
    scores = jnp.where(place < lengths[0], scores * scale, -jnp.inf)
    own = jnp.sum(query * new_latent, axis=1, keepdims=True)
    own = own + jnp.sum(rope.astype(F32) * new_key, axis=1, keepdims=True)
    own = own * scale
    peak = jnp.maximum(jnp.max(scores, axis=1, keepdims=True), own)
    cache_exp = jnp.exp(scores - peak)
    own_exp = jnp.exp(own - peak)
    total = jnp.sum(cache_exp, axis=1, keepdims=True) + own_exp
    probs = (cache_exp / total).astype(BF16)
    own_probs = (own_exp / total).astype(BF16).astype(F32)
    mixed = dot32(probs, cache) + own_probs * new_latent
    mixed = mixed.astype(BF16).astype(F32)
    heads = mixed.shape[0]
    even = lax.broadcasted_iota(jnp.int32, mixed.shape, 0) % 2 == 0
    first = jnp.where(even, mixed, pltpu.roll(mixed, 1, 0))
    second = jnp.where(even, pltpu.roll(mixed, heads - 1, 0), mixed)
    count = LATENT_UNITS // LANES
    for s in range(count):
        tile = slice(s * LANES, (s + 1) * LANES)
        out[:, s, :] = first[:, tile]
        out[:, count + s, :] = second[:, tile]


def tile_at(number):
    return pl.ds(pl.multiple_of(number * LANES, LANES), LANES)


def slot_rows(ids_t, slots):
    top, tokens = ids_t.shape
    place = lax.broadcasted_iota(jnp.int32, (slots, tokens), 0)
    hits = [ids_t[k : k + 1, :] == place // CAP for k in range(top)]
    named = jnp.zeros((slots, tokens), F32)
    for hit in hits:
        named = named + jnp.where(hit, 1.0, 0.0)
    i = lax.broadcasted_iota(jnp.int32, (tokens, tokens), 0)
    j = lax.broadcasted_iota(jnp.int32, (tokens, tokens), 1)
    before = dot32(named.astype(BF16), jnp.where(i < j, 1.0, 0.0).astype(BF16))
    return jnp.where(before == (place % CAP).astype(F32), named, 0.0), hits


def prepare_body(index, ids_t, weights_t, value_up, gain, w_output, pack, combine):
    other = 1 - index[0] % 2
    rows = value_up.shape[0]
    pack[:rows, :LATENT_UNITS] = value_up[...]
    for m in range(8):
        at = LATENT_UNITS + m * LANES
        pack[:rows, at : at + LANES] = w_output[:, tile_at(2 * m + other)]
    wide_gain = jnp.concatenate([row(gain), jnp.zeros((1, LANES - rows), F32)], axis=1)
    pack[rows:, :] = jnp.zeros((16, pack.shape[1]), BF16)
    pack[rows:, :LANES] = jnp.broadcast_to(wide_gain, (16, LANES)).astype(BF16)

    tokens = ids_t.shape[1]
    taken, hits = slot_rows(ids_t, combine.shape[1])
    total = jnp.zeros(taken.shape, F32)
    for k, hit in enumerate(hits):
        total = total + jnp.where(hit, weights_t[k : k + 1, :], 0.0)
    total = jnp.where(taken > 0.0, total, 0.0)
    i = lax.broadcasted_iota(jnp.int32, (tokens, tokens), 0)
    j = lax.broadcasted_iota(jnp.int32, (tokens, tokens), 1)
    unit = jnp.where(i == j, 1.0, 0.0).astype(BF16)
    for p in range(3):
        part = total.astype(BF16)
        combine[p * tokens : (p + 1) * tokens, :] = dot_t(unit, part).astype(BF16)
        total = total - part.astype(F32)


def head_values(values, value_up, gains):
    head = dot_t(values.astype(BF16), value_up)
    factor = lax.rsqrt(jnp.mean(head * head, axis=-1, keepdims=True) + EPS)
    return (head * factor * gains).astype(BF16)


def head_body(index, attended, value_up, gain, w_output, pack, out):
    core = index[0] % 2
    count = LATENT_UNITS // LANES
    first = jnp.concatenate([attended[:, s, :] for s in range(count)], axis=1)
    second = jnp.concatenate([attended[:, count + s, :] for s in range(count)], axis=1)
    rows = value_up.shape[0]
    own = head_values(jnp.where(core == 0, first, second), value_up[...], row(gain))
    gains = pack[rows:, :LANES].astype(F32)[:1, :rows]
    other = head_values(
        jnp.where(core == 0, second, first), pack[:rows, :LATENT_UNITS], gains
    )
    tokens = own.shape[0]
    shares = dot32(other, pack[:rows, LATENT_UNITS:])
    for m in range(8):
        share = dot32(own, w_output[:, tile_at(2 * m + core)])
        share = (share + shares[:, m * LANES : (m + 1) * LANES]).astype(BF16)
        for p in range(out.shape[0]):
            out[p, m * tokens : (m + 1) * tokens, :] = share


def middle_body(index, shares, hidden, ids_t, middle_out, out, wide):
    core = index[0] % 2
    peers = shares.shape[0]
    tokens = hidden.shape[0]
    slots = wide.shape[0] // 8
    dispatch = slot_rows(ids_t, slots)[0].astype(BF16)
    for m in range(8):
        at = slice(m * tokens, (m + 1) * tokens)
        total = shares[0, at, :].astype(F32)
        for p in range(1, peers):
            total = total + shares[p, at, :].astype(F32)
        middle = (hidden[:, tile_at(2 * m + core)].astype(F32) + total).astype(BF16)
        middle_out[at, :] = middle
        wide[pl.ds(m, slots, stride=8), :] = dot32(dispatch, middle)
    rows = out.shape[1]
    for p in range(out.shape[0]):
        out[p] = wide[p * rows : (p + 1) * rows, :].astype(BF16)


def side_body(
    index, middle, other, gain, w_gate, w_up, w_shared_down, w_dense_up, w_dense_down, gate,
    own_out, other_out,
):
    core = index[0] % 2
    tokens = middle.shape[0] // 8
    tiles = []
    for j in range(16):
        at = slice(j // 2 * tokens, (j // 2 + 1) * tokens)
        mine, theirs = middle[at, :].astype(F32), other[at, :].astype(F32)
        tiles.append(jnp.where(core == j % 2, mine, theirs))
    values = jnp.concatenate(tiles, axis=1)
    factor = lax.rsqrt(jnp.mean(values * values, axis=-1, keepdims=True) + EPS)
    x = (values * factor * row(gain)).astype(BF16)
    pre = dot_t(x, w_gate[...])
    shared = (pre / (1.0 + jnp.exp(-pre)) * dot_t(x, w_up[...])).astype(BF16)
    dense = jax.nn.gelu(dot32(x, w_dense_up[...])).astype(BF16)
    logit = jnp.sum(x.astype(F32) * row(gate), axis=1, keepdims=True)
    mix = 1.0 / (1.0 + jnp.exp(-logit))
    side = dot32(shared, w_shared_down[...]) + mix * dot32(dense, w_dense_down[...])
    for m in range(8):
        at = slice(m * tokens, (m + 1) * tokens)
        low = side[:, 2 * m * LANES : (2 * m + 1) * LANES]
        high = side[:, (2 * m + 1) * LANES : (2 * m + 2) * LANES]
        own_out[at, :] = jnp.where(core == 0, low, high)
        other_out[at, :] = jnp.where(core == 0, high, low)


def expert_body(
    index, arrived, other, gain, *refs,
):
    weights, (out, wide, wide_other, rows_in, gains, *held, sems) = refs[:6], refs[6:]
    copies = [
        pltpu.make_async_copy(weight.at[0], place, sems.at[k])
        for k, (weight, place) in enumerate(zip(weights, held))
    ]
    for copy in copies:
        copy.start()
    core = index[0] % 2
    peers, rows, _ = arrived.shape
    slots = peers * rows // 8
    gains[...] = row(gain)
    for p in range(peers):
        at = slice(p * rows, (p + 1) * rows)
        wide[at, :] = arrived[p].astype(F32)
        wide_other[at, :] = other[p].astype(F32)
    square = jnp.zeros((slots, LANES), F32)
    for m in range(8):
        mine = wide[pl.ds(m, slots, stride=8), :]
        theirs = wide_other[pl.ds(m, slots, stride=8), :]
        square = square + mine * mine + theirs * theirs
    mean = jnp.sum(square, axis=1, keepdims=True) * (1.0 / MODEL_WIDTH)
    factor = lax.rsqrt(mean + EPS)
    for m in range(8):
        for source, number in ((wide, 2 * m + core), (wide_other, 2 * m + 1 - core)):
            values = source[pl.ds(m, slots, stride=8), :]
            normed = values * factor * gains[:, tile_at(number)]
            rows_in[:, tile_at(number)] = normed.astype(BF16)
    x = rows_in[...]
    acts = []
    for gate, up in ((0, 1), (3, 4)):
        copies[gate].wait()
        pre = dot32(x, held[gate][...])
        copies[up].wait()
        acts.append((pre / (1.0 + jnp.exp(-pre)) * dot32(x, held[up][...])).astype(BF16))
    copies[2].wait()
    copies[5].wait()
    for m in range(8):
        at = tile_at(2 * m + core)
        part = dot32(acts[0], held[2][:, at]) + dot32(acts[1], held[5][:, at])
        wide[pl.ds(m, slots, stride=8), :] = part
    for p in range(peers):
        out[p] = wide[p * rows : (p + 1) * rows, :].astype(BF16)


def combine_body(returned, weights, side, out, wide):
    peers, rows, _ = returned.shape
    slots = peers * rows // 8
    tokens = side.shape[0] // 8
    for p in range(peers):
        wide[p * rows : (p + 1) * rows, :] = returned[p].astype(F32)
    for m in range(8):
        block = wide[pl.ds(m, slots, stride=8), :].astype(BF16)
        sums = dot32(weights[...], block)
        routed = sums[:tokens] + sums[tokens : 2 * tokens] + sums[2 * tokens :]
        at = slice(m * tokens, (m + 1) * tokens)
        out[m] = (routed + side[at, :]).astype(BF16)


def final_body(index, tiles, middle, out):
    total = tiles[0].astype(F32)
    for j in range(1, tiles.shape[0]):
        total = total + tiles[j].astype(F32)
    tokens = out.shape[0]
    start = pl.multiple_of(index[0] // 2 * tokens, tokens)
    out[...] = (middle[pl.ds(start, tokens), :].astype(F32) + total).astype(BF16)


def on_device(
    hidden,
    lengths,
    latent_cache,
    cache_rotary,
    attn_gain,
    w_query_nope,
    w_query_rope,
    latent_weight,
    w_rotary_key,
    latent_norm_gain,
    key_up_weight,
    value_up_weight,
    head_gain,
    w_output,
    ffn_gain,
    expert_ids,
    expert_weights,
    w_expert_gate,
    w_expert_up,
    w_expert_down,
    w_shared_gate,
    w_shared_up,
    w_shared_down,
    w_dense_up,
    w_dense_down,
    dense_gate,
):
    tp = lax.axis_size("tp")
    ep = lax.axis_size("ep")
    index = lax.axis_index("tp").astype(jnp.int32).reshape(1)
    tokens = hidden.shape[0]
    slots = ep * CAP
    places = latent_cache.shape[1]
    chips = tp // 2
    same_core = [list(range(core, tp, 2)) for core in range(2)]
    small = shape((tp, 8, LANES), F32)
    half = (chips * tokens, LANES)
    large = shape((ep, slots * chips // ep, LANES), BF16)
    wide = pltpu.VMEM((slots * chips, LANES), F32)

    payload, normed = call(
        query_body,
        (small, shape(hidden.shape, BF16)),
        (hidden, attn_gain, w_query_nope.T, w_query_rope.T, key_up_weight),
        hbm=range(5),
        leave=(0,),
    )
    queries = exchange(payload, "tp")

    inverse = 1.0 / 10000.0 ** (jnp.arange(HALF, dtype=F32) / HALF)
    angles = lengths.astype(F32)[:, None] * inverse[None, :]
    cos, sin = jnp.cos(angles), jnp.sin(angles)
    token, cache = call(
        new_token_body,
        (
            shape((1, LATENT_UNITS + LANES), F32),
            shape((places + places * ROPE // LATENT_UNITS, LATENT_UNITS), BF16),
        ),
        (
            index,
            normed,
            latent_weight,
            w_rotary_key.T,
            latent_norm_gain,
            cos,
            sin,
            latent_cache,
            cache_rotary,
        ),
        smem=(0,),
        hbm=(2, 3, 4, 5, 6),
        raw=(7, 8),
        scratch=(pltpu.SemaphoreType.DMA((1 + places // LATENT_UNITS,)),),
    )
    queries, token = together(queries, token)

    payload = call(
        attention_body,
        small,
        (lengths, queries, cache, token, cos, sin),
        smem=(0,),
        leave=(0,),
    )
    payload, later = together(payload, index)
    attended = exchange(payload, "tp")
    pack, combine = call(
        prepare_body,
        (
            shape((PLAIN_QUERY + 16, LATENT_UNITS + chips * LANES), BF16),
            shape((3 * tokens, slots), BF16),
        ),
        (later, expert_ids.T, expert_weights.T, value_up_weight.T, head_gain, w_output),
        smem=(0,),
        hbm=range(1, 6),
    )
    pack = core_swap(pack)
    attended, pack, combine = together(attended, pack, combine)

    payload = call(
        head_body,
        shape((chips,) + half, BF16),
        (index, attended, value_up_weight.T, head_gain, w_output, pack),
        smem=(0,),
        leave=(0,),
    )
    own_weights = (w_expert_gate, w_expert_up, w_expert_down)
    payload, *weights = together(payload, *own_weights)
    shares = exchange(payload, "tp", same_core)
    weights = [core_swap(w) for w in weights]
    shares, *weights = together(shares, *weights)

    middle, payload = call(
        middle_body,
        (shape(half, BF16), large),
        (index, shares, hidden, expert_ids.T),
        smem=(0,),
        scratch=(wide,),
        leave=(1,),
    )
    payload, later = together(payload, middle)
    arrived = exchange(payload, "ep")
    other = core_swap(later)
    arrived, other = together(arrived, other)
    payload = call(
        expert_body,
        large,
        (
            index,
            arrived,
            core_swap(arrived),
            ffn_gain,
            *own_weights,
            *weights,
        ),
        smem=(0,),
        raw=range(4, 10),
        leave=(0,),
        scratch=(
            wide,
            wide,
            pltpu.VMEM((slots, MODEL_WIDTH), BF16),
            pltpu.VMEM((1, MODEL_WIDTH), F32),
            *(pltpu.VMEM(w.shape[1:], BF16) for w in own_weights * 2),
            pltpu.SemaphoreType.DMA((6,)),
        ),
    )
    payload, later, other = together(payload, later, other)
    returned = exchange(payload, "ep")
    side, away = call(
        side_body,
        (shape(half, F32), shape(half, F32)),
        (
            index,
            later,
            other,
            ffn_gain,
            w_shared_gate.T,
            w_shared_up.T,
            w_shared_down,
            w_dense_up,
            w_dense_down,
            dense_gate,
        ),
        smem=(0,),
        hbm=range(3, 10),
        leave=(1,),
    )
    away = core_swap(away)
    returned, side = together(returned, side + away)

    payload = call(
        combine_body,
        shape((chips, tokens, LANES), BF16),
        (returned, combine, side),
        scratch=(wide,),
    )
    parts = exchange(payload, "tp", same_core)
    return call(
        final_body, shape((tokens, LANES), BF16), (index, parts, middle), smem=(0,), leave=(0,)
    )


def solution(mesh):
    placed = (
        P("ep", None),
        P(("ep", "tp")),
        P(("ep", "tp"), None, None),
        P(("ep", "tp"), None, None),
        P(),
        P(None, "tp"),
        P(None, "tp"),
        P(),
        P(),
        P(),
        P("tp", None),
        P(None, "tp"),
        P("tp"),
        P("tp", None),
        P(),
        P("ep", None),
        P("ep", None),
        P("ep", None, "tp"),
        P("ep", None, "tp"),
        P("ep", "tp", None),
        P(None, "tp"),
        P(None, "tp"),
        P("tp", None),
        P(None, "tp"),
        P("tp", None),
        P(),
    )
    return jax.shard_map(
        on_device, mesh=mesh, in_specs=placed, out_specs=P("ep", "tp"), check_vma=False
    )
```

```python
import jax
import jax.numpy as jnp
from jax import lax
from jax.experimental import pallas as pl
from jax.experimental.pallas import tpu as pltpu
from jax.sharding import PartitionSpec as P

MODEL_WIDTH = 2048
PLAIN_QUERY = 64
ROPE = 32
HALF = 16
LATENT_UNITS = 512
CAP = 2
LANES = 128
F32 = jnp.float32
BF16 = jnp.bfloat16
EPS = 1e-06


def exchange(x, axis, groups=None):
    return lax.all_to_all(
        x, axis, split_axis=0, concat_axis=0, axis_index_groups=groups, tiled=True
    )


def core_swap(x):
    return lax.ppermute(x, "tp", [(i, i ^ 1) for i in range(lax.axis_size("tp"))])


def dot32(a, b):
    return jnp.dot(a, b, preferred_element_type=F32)


def dot_t(a, b):
    return lax.dot_general(a, b, (((1,), (1,)), ((), ())), preferred_element_type=F32)


def call(body, outs, args, smem=(), hbm=(), raw=(), scratch=(), leave=()):
    vmem = pl.BlockSpec(memory_space=pltpu.VMEM)
    kinds = {i: pl.BlockSpec(memory_space=pltpu.SMEM) for i in smem}
    kinds.update({i: pl.BlockSpec(memory_space=pl.ANY) for i in raw})
    free = set(smem) | set(hbm) | set(raw)
    scalars = set(smem)
    args = [
        x
        if i in scalars
        else pltpu.with_memory_space_constraint(x, pltpu.HBM if i in free else pltpu.VMEM)
        for i, x in enumerate(args)
    ]
    leaves, tree = jax.tree.flatten(outs)
    outs = tree.unflatten(
        (pltpu.HBM if i in leave else pltpu.VMEM)(o.shape, o.dtype) for i, o in enumerate(leaves)
    )
    return pl.pallas_call(
        body,
        out_shape=outs,
        in_specs=[kinds.get(i, vmem) for i in range(len(args))],
        out_specs=tree.unflatten(vmem for _ in leaves),
        scratch_shapes=list(scratch),
        compiler_params=pltpu.CompilerParams(vmem_limit_bytes=16 * 1024 * 1024),
    )(*args)


def together(*values):
    return lax.optimization_barrier(values)


def shape(dims, dtype):
    return jax.ShapeDtypeStruct(dims, dtype)


def row(gain):
    return gain[...].astype(F32).reshape(1, -1)


def query_body(hidden, gain, w_nope, w_rope, key_up, out, normed_out):
    values = hidden[...].astype(F32)
    factor = lax.rsqrt(jnp.mean(values * values, axis=-1, keepdims=True) + EPS)
    normed = (values * factor * row(gain)).astype(BF16)
    normed_out[...] = normed
    nope = dot_t(normed, w_nope[...]).astype(BF16)
    rope = dot_t(normed, w_rope[...]).astype(BF16).astype(F32)
    latent = dot32(nope, key_up[...]).astype(BF16).astype(F32)
    for s in range(LATENT_UNITS // LANES):
        out[:, s, :] = latent[:, s * LANES : (s + 1) * LANES]
    rows = out.shape[0]
    out[:, 4, :] = jnp.concatenate([rope, jnp.zeros((rows, LANES - ROPE), F32)], axis=1)
    for s in range(5, 8):
        out[:, s, :] = jnp.zeros((rows, LANES), F32)


def rotated(values, cos, sin):
    first, second = values[:, :HALF], values[:, HALF:ROPE]
    return jnp.concatenate([first * cos - second * sin, first * sin + second * cos], axis=1)


def new_token_body(
    index, normed, w_latent, w_key, gain, cos, sin, cache, rotary, out, cache_out, sems
):
    places, width = cache.shape[1:]
    copies = [pltpu.make_async_copy(cache.at[0], cache_out.at[pl.ds(0, places)], sems.at[0])]
    for k in range(rotary.shape[2] // width):
        source = rotary.at[0, :, pl.ds(k * width, width)]
        target = cache_out.at[pl.ds(places + k * ROPE, ROPE)]
        copies.append(pltpu.make_async_copy(source, target, sems.at[k + 1]))
    for copy in copies:
        copy.start()
    latent = dot32(normed[...], w_latent[...])
    key = dot_t(normed[...], w_key[...])
    rows = lax.broadcasted_iota(jnp.int32, (latent.shape[0], 1), 0)
    mine = rows == index[0]
    latent = jnp.sum(jnp.where(mine, latent, 0.0), axis=0, keepdims=True)
    key = jnp.sum(jnp.where(mine, key, 0.0), axis=0, keepdims=True)
    factor = lax.rsqrt(jnp.mean(latent * latent, axis=-1, keepdims=True) + EPS)
    out[:, :LATENT_UNITS] = (latent * factor * row(gain)).astype(BF16).astype(F32)
    key = rotated(key, cos[...], sin[...]).astype(BF16).astype(F32)
    out[:, LATENT_UNITS:] = jnp.concatenate([key, jnp.zeros((1, LANES - ROPE), F32)], axis=1)
    for copy in copies:
        copy.wait()


def attention_body(lengths, queries, caches, token, cos, sin, out):
    new_latent = token[:, :LATENT_UNITS]
    new_key = token[:, LATENT_UNITS : LATENT_UNITS + ROPE]
    parts = [queries[:, s, :] for s in range(LATENT_UNITS // LANES)]
    query = jnp.concatenate(parts, axis=1)
    rope = rotated(queries[:, 4, :], cos[...], sin[...]).astype(BF16)
    scale = (PLAIN_QUERY + ROPE) ** (-0.5)
    count = caches.shape[0] * LATENT_UNITS // (LATENT_UNITS + ROPE)
    cache = caches[:count, :]
    turned = [
        dot32(rope, caches[count + k * ROPE : count + (k + 1) * ROPE, :])
        for k in range(count // LATENT_UNITS)
    ]
    scores = dot_t(query.astype(BF16), cache) + jnp.concatenate(turned, axis=1)
    place = lax.broadcasted_iota(jnp.int32, scores.shape, 1)
    scores = jnp.where(place < lengths[0], scores * scale, -jnp.inf)
    own = jnp.sum(query * new_latent, axis=1, keepdims=True)
    own = own + jnp.sum(rope.astype(F32) * new_key, axis=1, keepdims=True)
    own = own * scale
    peak = jnp.maximum(jnp.max(scores, axis=1, keepdims=True), own)
    cache_exp = jnp.exp(scores - peak)
    own_exp = jnp.exp(own - peak)
    total = jnp.sum(cache_exp, axis=1, keepdims=True) + own_exp
    probs = (cache_exp / total).astype(BF16)
    own_probs = (own_exp / total).astype(BF16).astype(F32)
    mixed = dot32(probs, cache) + own_probs * new_latent
    mixed = mixed.astype(BF16).astype(F32)
    heads = mixed.shape[0]
    even = lax.broadcasted_iota(jnp.int32, mixed.shape, 0) % 2 == 0
    first = jnp.where(even, mixed, pltpu.roll(mixed, 1, 0))
    second = jnp.where(even, pltpu.roll(mixed, heads - 1, 0), mixed)
    count = LATENT_UNITS // LANES
    for s in range(count):
        tile = slice(s * LANES, (s + 1) * LANES)
        out[:, s, :] = first[:, tile]
        out[:, count + s, :] = second[:, tile]


def tile_at(number):
    return pl.ds(pl.multiple_of(number * LANES, LANES), LANES)


def slot_rows(ids_t, slots):
    top, tokens = ids_t.shape
    place = lax.broadcasted_iota(jnp.int32, (slots, tokens), 0)
    hits = [ids_t[k : k + 1, :] == place // CAP for k in range(top)]
    named = jnp.zeros((slots, tokens), F32)
    for hit in hits:
        named = named + jnp.where(hit, 1.0, 0.0)
    i = lax.broadcasted_iota(jnp.int32, (tokens, tokens), 0)
    j = lax.broadcasted_iota(jnp.int32, (tokens, tokens), 1)
    before = dot32(named.astype(BF16), jnp.where(i < j, 1.0, 0.0).astype(BF16))
    return jnp.where(before == (place % CAP).astype(F32), named, 0.0), hits


def prepare_body(index, ids_t, weights_t, value_up, gain, w_output, pack, combine):
    other = 1 - index[0] % 2
    rows = value_up.shape[0]
    pack[:rows, :LATENT_UNITS] = value_up[...]
    for m in range(8):
        at = LATENT_UNITS + m * LANES
        pack[:rows, at : at + LANES] = w_output[:, tile_at(2 * m + other)]
    wide_gain = jnp.concatenate([row(gain), jnp.zeros((1, LANES - rows), F32)], axis=1)
    pack[rows:, :] = jnp.zeros((16, pack.shape[1]), BF16)
    pack[rows:, :LANES] = jnp.broadcast_to(wide_gain, (16, LANES)).astype(BF16)

    tokens = ids_t.shape[1]
    taken, hits = slot_rows(ids_t, combine.shape[1])
    total = jnp.zeros(taken.shape, F32)
    for k, hit in enumerate(hits):
        total = total + jnp.where(hit, weights_t[k : k + 1, :], 0.0)
    total = jnp.where(taken > 0.0, total, 0.0)
    i = lax.broadcasted_iota(jnp.int32, (tokens, tokens), 0)
    j = lax.broadcasted_iota(jnp.int32, (tokens, tokens), 1)
    unit = jnp.where(i == j, 1.0, 0.0).astype(BF16)
    for p in range(3):
        part = total.astype(BF16)
        combine[p * tokens : (p + 1) * tokens, :] = dot_t(unit, part).astype(BF16)
        total = total - part.astype(F32)


def head_values(values, value_up, gains):
    head = dot_t(values.astype(BF16), value_up)
    factor = lax.rsqrt(jnp.mean(head * head, axis=-1, keepdims=True) + EPS)
    return (head * factor * gains).astype(BF16)


def head_body(index, attended, value_up, gain, w_output, pack, out):
    core = index[0] % 2
    count = LATENT_UNITS // LANES
    first = jnp.concatenate([attended[:, s, :] for s in range(count)], axis=1)
    second = jnp.concatenate([attended[:, count + s, :] for s in range(count)], axis=1)
    rows = value_up.shape[0]
    own = head_values(jnp.where(core == 0, first, second), value_up[...], row(gain))
    gains = pack[rows:, :LANES].astype(F32)[:1, :rows]
    other = head_values(
        jnp.where(core == 0, second, first), pack[:rows, :LATENT_UNITS], gains
    )
    tokens = own.shape[0]
    shares = dot32(other, pack[:rows, LATENT_UNITS:])
    for m in range(8):
        share = dot32(own, w_output[:, tile_at(2 * m + core)])
        share = (share + shares[:, m * LANES : (m + 1) * LANES]).astype(BF16)
        for p in range(out.shape[0]):
            out[p, m * tokens : (m + 1) * tokens, :] = share


def middle_body(index, shares, hidden, ids_t, middle_out, out, wide):
    core = index[0] % 2
    peers = shares.shape[0]
    tokens = hidden.shape[0]
    slots = wide.shape[0] // 8
    dispatch = slot_rows(ids_t, slots)[0].astype(BF16)
    for m in range(8):
        at = slice(m * tokens, (m + 1) * tokens)
        total = shares[0, at, :].astype(F32)
        for p in range(1, peers):
            total = total + shares[p, at, :].astype(F32)
        middle = (hidden[:, tile_at(2 * m + core)].astype(F32) + total).astype(BF16)
        middle_out[at, :] = middle
        wide[pl.ds(m, slots, stride=8), :] = dot32(dispatch, middle)
    rows = out.shape[1]
    for p in range(out.shape[0]):
        out[p] = wide[p * rows : (p + 1) * rows, :].astype(BF16)


def side_body(
    index, middle, other, gain, w_gate, w_up, w_shared_down, w_dense_up, w_dense_down, gate,
    own_out, other_out,
):
    core = index[0] % 2
    tokens = middle.shape[0] // 8
    tiles = []
    for j in range(16):
        at = slice(j // 2 * tokens, (j // 2 + 1) * tokens)
        mine, theirs = middle[at, :].astype(F32), other[at, :].astype(F32)
        tiles.append(jnp.where(core == j % 2, mine, theirs))
    values = jnp.concatenate(tiles, axis=1)
    factor = lax.rsqrt(jnp.mean(values * values, axis=-1, keepdims=True) + EPS)
    x = (values * factor * row(gain)).astype(BF16)
    pre = dot_t(x, w_gate[...])
    shared = (pre / (1.0 + jnp.exp(-pre)) * dot_t(x, w_up[...])).astype(BF16)
    dense = jax.nn.gelu(dot32(x, w_dense_up[...])).astype(BF16)
    logit = jnp.sum(x.astype(F32) * row(gate), axis=1, keepdims=True)
    mix = 1.0 / (1.0 + jnp.exp(-logit))
    side = dot32(shared, w_shared_down[...]) + mix * dot32(dense, w_dense_down[...])
    for m in range(8):
        at = slice(m * tokens, (m + 1) * tokens)
        low = side[:, 2 * m * LANES : (2 * m + 1) * LANES]
        high = side[:, (2 * m + 1) * LANES : (2 * m + 2) * LANES]
        own_out[at, :] = jnp.where(core == 0, low, high)
        other_out[at, :] = jnp.where(core == 0, high, low)


def expert_body(
    index, arrived, other, gain, *refs,
):
    weights, (out, wide, wide_other, rows_in, gains, own_in, other_in, down, sems) = (
        refs[:6],
        refs[6:],
    )
    core = index[0] % 2
    width = weights[0].shape[2]
    pairs = []
    for block, place in ((0, own_in), (1, other_in)):
        for k in range(2):
            target = place.at[:, pl.ds(k * width, width)]
            pairs.append((weights[3 * block + k].at[0], target))
    for block in range(2):
        for m in range(8):
            source = weights[3 * block + 2].at[0, :, tile_at(2 * m + core)]
            target = down.at[pl.ds(block * width, width), pl.ds(m * LANES, LANES)]
            pairs.append((source, target))
    copies = [pltpu.make_async_copy(*pair, sems.at[k]) for k, pair in enumerate(pairs)]
    for copy in copies:
        copy.start()
    peers, rows, _ = arrived.shape
    slots = peers * rows // 8
    gains[...] = row(gain)
    for p in range(peers):
        at = slice(p * rows, (p + 1) * rows)
        wide[at, :] = arrived[p].astype(F32)
        wide_other[at, :] = other[p].astype(F32)
    square = jnp.zeros((slots, LANES), F32)
    for m in range(8):
        mine = wide[pl.ds(m, slots, stride=8), :]
        theirs = wide_other[pl.ds(m, slots, stride=8), :]
        square = square + mine * mine + theirs * theirs
    mean = jnp.sum(square, axis=1, keepdims=True) * (1.0 / MODEL_WIDTH)
    factor = lax.rsqrt(mean + EPS)
    for m in range(8):
        for source, number in ((wide, 2 * m + core), (wide_other, 2 * m + 1 - core)):
            values = source[pl.ds(m, slots, stride=8), :]
            normed = values * factor * gains[:, tile_at(number)]
            rows_in[:, tile_at(number)] = normed.astype(BF16)
    x = rows_in[...]
    acts = []
    for block, place in ((0, own_in), (1, other_in)):
        copies[2 * block].wait()
        copies[2 * block + 1].wait()
        both = dot32(x, place[...])
        pre = both[:, :width]
        acts.append((pre / (1.0 + jnp.exp(-pre)) * both[:, width:]).astype(BF16))
    for copy in copies[4:]:
        copy.wait()
    part = dot32(jnp.concatenate(acts, axis=1), down[...])
    for m in range(8):
        wide[pl.ds(m, slots, stride=8), :] = part[:, m * LANES : (m + 1) * LANES]
    for p in range(peers):
        out[p] = wide[p * rows : (p + 1) * rows, :].astype(BF16)


def combine_body(returned, weights, side, out, wide):
    peers, rows, _ = returned.shape
    slots = peers * rows // 8
    tokens = side.shape[0] // 8
    for p in range(peers):
        wide[p * rows : (p + 1) * rows, :] = returned[p].astype(F32)
    for m in range(8):
        block = wide[pl.ds(m, slots, stride=8), :].astype(BF16)
        sums = dot32(weights[...], block)
        routed = sums[:tokens] + sums[tokens : 2 * tokens] + sums[2 * tokens :]
        at = slice(m * tokens, (m + 1) * tokens)
        out[m] = (routed + side[at, :]).astype(BF16)


def final_body(index, tiles, middle, out):
    total = tiles[0].astype(F32)
    for j in range(1, tiles.shape[0]):
        total = total + tiles[j].astype(F32)
    tokens = out.shape[0]
    start = pl.multiple_of(index[0] // 2 * tokens, tokens)
    out[...] = (middle[pl.ds(start, tokens), :].astype(F32) + total).astype(BF16)


def on_device(
    hidden,
    lengths,
    latent_cache,
    cache_rotary,
    attn_gain,
    w_query_nope,
    w_query_rope,
    latent_weight,
    w_rotary_key,
    latent_norm_gain,
    key_up_weight,
    value_up_weight,
    head_gain,
    w_output,
    ffn_gain,
    expert_ids,
    expert_weights,
    w_expert_gate,
    w_expert_up,
    w_expert_down,
    w_shared_gate,
    w_shared_up,
    w_shared_down,
    w_dense_up,
    w_dense_down,
    dense_gate,
):
    tp = lax.axis_size("tp")
    ep = lax.axis_size("ep")
    index = lax.axis_index("tp").astype(jnp.int32).reshape(1)
    tokens = hidden.shape[0]
    slots = ep * CAP
    places = latent_cache.shape[1]
    chips = tp // 2
    same_core = [list(range(core, tp, 2)) for core in range(2)]
    small = shape((tp, 8, LANES), F32)
    half = (chips * tokens, LANES)
    large = shape((ep, slots * chips // ep, LANES), BF16)
    wide = pltpu.VMEM((slots * chips, LANES), F32)

    payload, normed = call(
        query_body,
        (small, shape(hidden.shape, BF16)),
        (hidden, attn_gain, w_query_nope.T, w_query_rope.T, key_up_weight),
        hbm=range(5),
        leave=(0,),
    )
    queries = exchange(payload, "tp")

    inverse = 1.0 / 10000.0 ** (jnp.arange(HALF, dtype=F32) / HALF)
    angles = lengths.astype(F32)[:, None] * inverse[None, :]
    cos, sin = jnp.cos(angles), jnp.sin(angles)
    token, cache = call(
        new_token_body,
        (
            shape((1, LATENT_UNITS + LANES), F32),
            shape((places + places * ROPE // LATENT_UNITS, LATENT_UNITS), BF16),
        ),
        (
            index,
            normed,
            latent_weight,
            w_rotary_key.T,
            latent_norm_gain,
            cos,
            sin,
            latent_cache,
            cache_rotary,
        ),
        smem=(0,),
        hbm=(2, 3, 4, 5, 6),
        raw=(7, 8),
        scratch=(pltpu.SemaphoreType.DMA((1 + places // LATENT_UNITS,)),),
    )
    queries, token = together(queries, token)

    payload = call(
        attention_body,
        small,
        (lengths, queries, cache, token, cos, sin),
        smem=(0,),
        leave=(0,),
    )
    payload, later = together(payload, index)
    attended = exchange(payload, "tp")
    pack, combine = call(
        prepare_body,
        (
            shape((PLAIN_QUERY + 16, LATENT_UNITS + chips * LANES), BF16),
            shape((3 * tokens, slots), BF16),
        ),
        (later, expert_ids.T, expert_weights.T, value_up_weight.T, head_gain, w_output),
        smem=(0,),
        hbm=range(1, 6),
    )
    pack = core_swap(pack)
    attended, pack, combine = together(attended, pack, combine)

    payload = call(
        head_body,
        shape((chips,) + half, BF16),
        (index, attended, value_up_weight.T, head_gain, w_output, pack),
        smem=(0,),
    )
    shares = exchange(payload, "tp", same_core)

    middle, payload = call(
        middle_body,
        (shape(half, BF16), large),
        (index, shares, hidden, expert_ids.T),
        smem=(0,),
        scratch=(wide,),
        leave=(1,),
    )
    own_weights = (w_expert_gate, w_expert_up, w_expert_down)
    payload, later, *weights = together(payload, middle, *own_weights)
    arrived = exchange(payload, "ep")
    weights = [core_swap(w) for w in weights]
    arrived, *weights = together(arrived, *weights)
    payload = call(
        expert_body,
        large,
        (
            index,
            arrived,
            core_swap(arrived),
            ffn_gain,
            *own_weights,
            *weights,
        ),
        smem=(0,),
        raw=range(4, 10),
        leave=(0,),
        scratch=(
            wide,
            wide,
            pltpu.VMEM((slots, MODEL_WIDTH), BF16),
            pltpu.VMEM((1, MODEL_WIDTH), F32),
            pltpu.VMEM((MODEL_WIDTH, 2 * w_expert_gate.shape[2]), BF16),
            pltpu.VMEM((MODEL_WIDTH, 2 * w_expert_gate.shape[2]), BF16),
            pltpu.VMEM((2 * w_expert_down.shape[1], chips * LANES), BF16),
            pltpu.SemaphoreType.DMA((4 + 2 * chips,)),
        ),
    )
    payload, later = together(payload, later)
    returned = exchange(payload, "ep")
    other = core_swap(later)
    side, away = call(
        side_body,
        (shape(half, F32), shape(half, F32)),
        (
            index,
            later,
            other,
            ffn_gain,
            w_shared_gate.T,
            w_shared_up.T,
            w_shared_down,
            w_dense_up,
            w_dense_down,
            dense_gate,
        ),
        smem=(0,),
        hbm=range(3, 10),
        leave=(1,),
    )
    away = core_swap(away)
    returned, side = together(returned, side + away)

    payload = call(
        combine_body,
        shape((chips, tokens, LANES), BF16),
        (returned, combine, side),
        scratch=(wide,),
    )
    parts = exchange(payload, "tp", same_core)
    return call(
        final_body, shape((tokens, LANES), BF16), (index, parts, middle), smem=(0,), leave=(0,)
    )


def solution(mesh):
    placed = (
        P("ep", None),
        P(("ep", "tp")),
        P(("ep", "tp"), None, None),
        P(("ep", "tp"), None, None),
        P(),
        P(None, "tp"),
        P(None, "tp"),
        P(),
        P(),
        P(),
        P("tp", None),
        P(None, "tp"),
        P("tp"),
        P("tp", None),
        P(),
        P("ep", None),
        P("ep", None),
        P("ep", None, "tp"),
        P("ep", None, "tp"),
        P("ep", "tp", None),
        P(None, "tp"),
        P(None, "tp"),
        P("tp", None),
        P(None, "tp"),
        P("tp", None),
        P(),
    )
    return jax.shard_map(
        on_device, mesh=mesh, in_specs=placed, out_specs=P("ep", "tp"), check_vma=False
    )
```

```python
import jax
import jax.numpy as jnp
from jax import lax
from jax.experimental import pallas as pl
from jax.experimental.pallas import tpu as pltpu
from jax.sharding import PartitionSpec as P

MODEL_WIDTH = 2048
PLAIN_QUERY = 64
ROPE = 32
HALF = 16
LATENT_UNITS = 512
CAP = 2
LANES = 128
F32 = jnp.float32
BF16 = jnp.bfloat16
EPS = 1e-06


def exchange(x, axis, groups=None):
    return lax.all_to_all(
        x, axis, split_axis=0, concat_axis=0, axis_index_groups=groups, tiled=True
    )


def core_swap(x):
    return lax.ppermute(x, "tp", [(i, i ^ 1) for i in range(lax.axis_size("tp"))])


def dot32(a, b):
    return jnp.dot(a, b, preferred_element_type=F32)


def dot_t(a, b):
    return lax.dot_general(a, b, (((1,), (1,)), ((), ())), preferred_element_type=F32)


def call(body, outs, args, smem=(), hbm=(), raw=(), scratch=(), leave=()):
    vmem = pl.BlockSpec(memory_space=pltpu.VMEM)
    kinds = {i: pl.BlockSpec(memory_space=pltpu.SMEM) for i in smem}
    kinds.update({i: pl.BlockSpec(memory_space=pl.ANY) for i in raw})
    free = set(smem) | set(hbm) | set(raw)
    scalars = set(smem)
    args = [
        x
        if i in scalars
        else pltpu.with_memory_space_constraint(x, pltpu.HBM if i in free else pltpu.VMEM)
        for i, x in enumerate(args)
    ]
    leaves, tree = jax.tree.flatten(outs)
    outs = tree.unflatten(
        (pltpu.HBM if i in leave else pltpu.VMEM)(o.shape, o.dtype) for i, o in enumerate(leaves)
    )
    return pl.pallas_call(
        body,
        out_shape=outs,
        in_specs=[kinds.get(i, vmem) for i in range(len(args))],
        out_specs=tree.unflatten(vmem for _ in leaves),
        scratch_shapes=list(scratch),
        compiler_params=pltpu.CompilerParams(vmem_limit_bytes=16 * 1024 * 1024),
    )(*args)


def together(*values):
    return lax.optimization_barrier(values)


def shape(dims, dtype):
    return jax.ShapeDtypeStruct(dims, dtype)


def row(gain):
    return gain[...].astype(F32).reshape(1, -1)


def query_body(hidden, gain, w_nope, w_rope, key_up, out, normed_out):
    values = hidden[...].astype(F32)
    factor = lax.rsqrt(jnp.mean(values * values, axis=-1, keepdims=True) + EPS)
    normed = (values * factor * row(gain)).astype(BF16)
    normed_out[...] = normed
    nope = dot_t(normed, w_nope[...]).astype(BF16)
    rope = dot_t(normed, w_rope[...]).astype(BF16).astype(F32)
    latent = dot32(nope, key_up[...]).astype(BF16).astype(F32)
    for s in range(LATENT_UNITS // LANES):
        out[:, s, :] = latent[:, s * LANES : (s + 1) * LANES]
    rows = out.shape[0]
    out[:, 4, :] = jnp.concatenate([rope, jnp.zeros((rows, LANES - ROPE), F32)], axis=1)
    for s in range(5, 8):
        out[:, s, :] = jnp.zeros((rows, LANES), F32)


def rotated(values, cos, sin):
    first, second = values[:, :HALF], values[:, HALF:ROPE]
    return jnp.concatenate([first * cos - second * sin, first * sin + second * cos], axis=1)


def new_token_body(
    index, normed, w_latent, w_key, gain, cos, sin, cache, rotary, out, cache_out, sems
):
    places, width = cache.shape[1:]
    copies = [pltpu.make_async_copy(cache.at[0], cache_out.at[pl.ds(0, places)], sems.at[0])]
    for k in range(rotary.shape[2] // width):
        source = rotary.at[0, :, pl.ds(k * width, width)]
        target = cache_out.at[pl.ds(places + k * ROPE, ROPE)]
        copies.append(pltpu.make_async_copy(source, target, sems.at[k + 1]))
    for copy in copies:
        copy.start()
    latent = dot32(normed[...], w_latent[...])
    key = dot_t(normed[...], w_key[...])
    rows = lax.broadcasted_iota(jnp.int32, (latent.shape[0], 1), 0)
    mine = rows == index[0]
    latent = jnp.sum(jnp.where(mine, latent, 0.0), axis=0, keepdims=True)
    key = jnp.sum(jnp.where(mine, key, 0.0), axis=0, keepdims=True)
    factor = lax.rsqrt(jnp.mean(latent * latent, axis=-1, keepdims=True) + EPS)
    out[:, :LATENT_UNITS] = (latent * factor * row(gain)).astype(BF16).astype(F32)
    key = rotated(key, cos[...], sin[...]).astype(BF16).astype(F32)
    out[:, LATENT_UNITS:] = jnp.concatenate([key, jnp.zeros((1, LANES - ROPE), F32)], axis=1)
    for copy in copies:
        copy.wait()


def attention_body(lengths, queries, caches, token, cos, sin, out):
    new_latent = token[:, :LATENT_UNITS]
    new_key = token[:, LATENT_UNITS : LATENT_UNITS + ROPE]
    parts = [queries[:, s, :] for s in range(LATENT_UNITS // LANES)]
    query = jnp.concatenate(parts, axis=1)
    rope = rotated(queries[:, 4, :], cos[...], sin[...]).astype(BF16)
    scale = (PLAIN_QUERY + ROPE) ** (-0.5)
    count = caches.shape[0] * LATENT_UNITS // (LATENT_UNITS + ROPE)
    cache = caches[:count, :]
    turned = [
        dot32(rope, caches[count + k * ROPE : count + (k + 1) * ROPE, :])
        for k in range(count // LATENT_UNITS)
    ]
    scores = dot_t(query.astype(BF16), cache) + jnp.concatenate(turned, axis=1)
    place = lax.broadcasted_iota(jnp.int32, scores.shape, 1)
    scores = jnp.where(place < lengths[0], scores * scale, -jnp.inf)
    own = jnp.sum(query * new_latent, axis=1, keepdims=True)
    own = own + jnp.sum(rope.astype(F32) * new_key, axis=1, keepdims=True)
    own = own * scale
    peak = jnp.maximum(jnp.max(scores, axis=1, keepdims=True), own)
    cache_exp = jnp.exp(scores - peak)
    own_exp = jnp.exp(own - peak)
    total = jnp.sum(cache_exp, axis=1, keepdims=True) + own_exp
    probs = (cache_exp / total).astype(BF16)
    own_probs = (own_exp / total).astype(BF16).astype(F32)
    mixed = dot32(probs, cache) + own_probs * new_latent
    mixed = mixed.astype(BF16).astype(F32)
    heads = mixed.shape[0]
    even = lax.broadcasted_iota(jnp.int32, mixed.shape, 0) % 2 == 0
    first = jnp.where(even, mixed, pltpu.roll(mixed, 1, 0))
    second = jnp.where(even, pltpu.roll(mixed, heads - 1, 0), mixed)
    count = LATENT_UNITS // LANES
    for s in range(count):
        tile = slice(s * LANES, (s + 1) * LANES)
        out[:, s, :] = first[:, tile]
        out[:, count + s, :] = second[:, tile]


def tile_at(number):
    return pl.ds(pl.multiple_of(number * LANES, LANES), LANES)


def slot_rows(ids_t, slots):
    top, tokens = ids_t.shape
    place = lax.broadcasted_iota(jnp.int32, (slots, tokens), 0)
    hits = [ids_t[k : k + 1, :] == place // CAP for k in range(top)]
    named = jnp.zeros((slots, tokens), F32)
    for hit in hits:
        named = named + jnp.where(hit, 1.0, 0.0)
    i = lax.broadcasted_iota(jnp.int32, (tokens, tokens), 0)
    j = lax.broadcasted_iota(jnp.int32, (tokens, tokens), 1)
    before = dot32(named.astype(BF16), jnp.where(i < j, 1.0, 0.0).astype(BF16))
    return jnp.where(before == (place % CAP).astype(F32), named, 0.0), hits


def prepare_body(index, ids_t, weights_t, value_up, gain, w_output, pack, combine):
    other = 1 - index[0] % 2
    rows = value_up.shape[0]
    pack[:rows, :LATENT_UNITS] = value_up[...]
    for m in range(8):
        at = LATENT_UNITS + m * LANES
        pack[:rows, at : at + LANES] = w_output[:, tile_at(2 * m + other)]
    wide_gain = jnp.concatenate([row(gain), jnp.zeros((1, LANES - rows), F32)], axis=1)
    pack[rows:, :] = jnp.zeros((16, pack.shape[1]), BF16)
    pack[rows:, :LANES] = jnp.broadcast_to(wide_gain, (16, LANES)).astype(BF16)

    tokens = ids_t.shape[1]
    taken, hits = slot_rows(ids_t, combine.shape[1])
    total = jnp.zeros(taken.shape, F32)
    for k, hit in enumerate(hits):
        total = total + jnp.where(hit, weights_t[k : k + 1, :], 0.0)
    total = jnp.where(taken > 0.0, total, 0.0)
    i = lax.broadcasted_iota(jnp.int32, (tokens, tokens), 0)
    j = lax.broadcasted_iota(jnp.int32, (tokens, tokens), 1)
    unit = jnp.where(i == j, 1.0, 0.0).astype(BF16)
    for p in range(3):
        part = total.astype(BF16)
        combine[p * tokens : (p + 1) * tokens, :] = dot_t(unit, part).astype(BF16)
        total = total - part.astype(F32)


def head_values(values, value_up, gains):
    head = dot_t(values.astype(BF16), value_up)
    factor = lax.rsqrt(jnp.mean(head * head, axis=-1, keepdims=True) + EPS)
    return (head * factor * gains).astype(BF16)


def head_body(index, attended, value_up, gain, w_output, pack, out):
    core = index[0] % 2
    count = LATENT_UNITS // LANES
    first = jnp.concatenate([attended[:, s, :] for s in range(count)], axis=1)
    second = jnp.concatenate([attended[:, count + s, :] for s in range(count)], axis=1)
    rows = value_up.shape[0]
    own = head_values(jnp.where(core == 0, first, second), value_up[...], row(gain))
    gains = pack[rows:, :LANES].astype(F32)[:1, :rows]
    other = head_values(
        jnp.where(core == 0, second, first), pack[:rows, :LATENT_UNITS], gains
    )
    tokens = own.shape[0]
    shares = dot32(other, pack[:rows, LATENT_UNITS:])
    for m in range(8):
        share = dot32(own, w_output[:, tile_at(2 * m + core)])
        share = (share + shares[:, m * LANES : (m + 1) * LANES]).astype(BF16)
        for p in range(out.shape[0]):
            out[p, m * tokens : (m + 1) * tokens, :] = share


def middle_body(index, shares, hidden, ids_t, middle_out, out, wide):
    core = index[0] % 2
    peers = shares.shape[0]
    tokens = hidden.shape[0]
    slots = wide.shape[0] // 8
    dispatch = slot_rows(ids_t, slots)[0].astype(BF16)
    for m in range(8):
        at = slice(m * tokens, (m + 1) * tokens)
        total = shares[0, at, :].astype(F32)
        for p in range(1, peers):
            total = total + shares[p, at, :].astype(F32)
        middle = (hidden[:, tile_at(2 * m + core)].astype(F32) + total).astype(BF16)
        middle_out[at, :] = middle
        wide[pl.ds(m, slots, stride=8), :] = dot32(dispatch, middle)
    rows = out.shape[1]
    for p in range(out.shape[0]):
        out[p] = wide[p * rows : (p + 1) * rows, :].astype(BF16)


def side_body(
    index, middle, other, gain, w_gate, w_up, w_shared_down, w_dense_up, w_dense_down, gate,
    own_out, other_out,
):
    core = index[0] % 2
    tokens = middle.shape[0] // 8
    tiles = []
    for j in range(16):
        at = slice(j // 2 * tokens, (j // 2 + 1) * tokens)
        mine, theirs = middle[at, :].astype(F32), other[at, :].astype(F32)
        tiles.append(jnp.where(core == j % 2, mine, theirs))
    values = jnp.concatenate(tiles, axis=1)
    factor = lax.rsqrt(jnp.mean(values * values, axis=-1, keepdims=True) + EPS)
    x = (values * factor * row(gain)).astype(BF16)
    pre = dot_t(x, w_gate[...])
    shared = (pre / (1.0 + jnp.exp(-pre)) * dot_t(x, w_up[...])).astype(BF16)
    dense = jax.nn.gelu(dot32(x, w_dense_up[...])).astype(BF16)
    logit = jnp.sum(x.astype(F32) * row(gate), axis=1, keepdims=True)
    mix = 1.0 / (1.0 + jnp.exp(-logit))
    side = dot32(shared, w_shared_down[...]) + mix * dot32(dense, w_dense_down[...])
    for m in range(8):
        at = slice(m * tokens, (m + 1) * tokens)
        low = side[:, 2 * m * LANES : (2 * m + 1) * LANES]
        high = side[:, (2 * m + 1) * LANES : (2 * m + 2) * LANES]
        own_out[at, :] = jnp.where(core == 0, low, high)
        other_out[at, :] = jnp.where(core == 0, high, low)


def pack_body(index, w_gate, w_up, w_down, packed, down, sems):
    core = index[0] % 2
    depth, width = w_gate.shape[1:]
    pairs = [
        (w.at[0], packed.at[pl.ds(0, depth), pl.ds(k * width, width)])
        for k, w in enumerate((w_gate, w_up))
    ]
    for place, base, parity in ((packed, depth, 1 - core), (down, 0, core)):
        for m in range(8):
            block = pl.ds(base + m // 2 * width, width), pl.ds(m % 2 * LANES, LANES)
            pairs.append((w_down.at[0, :, tile_at(2 * m + parity)], place.at[block]))
    copies = [pltpu.make_async_copy(*pair, sems.at[k]) for k, pair in enumerate(pairs)]
    for copy in copies:
        copy.start()
    for copy in copies:
        copy.wait()


def expert_body(
    index, arrived, other, gain, packed, down, away, out, wide, wide_other, rows_in, gains
):
    core = index[0] % 2
    depth = packed.shape[0] - down.shape[0]
    width = down.shape[0] // 4
    peers, rows, _ = arrived.shape
    slots = peers * rows // 8
    gains[...] = row(gain)
    for p in range(peers):
        at = slice(p * rows, (p + 1) * rows)
        wide[at, :] = arrived[p].astype(F32)
        wide_other[at, :] = other[p].astype(F32)
    square = jnp.zeros((slots, LANES), F32)
    for m in range(8):
        mine = wide[pl.ds(m, slots, stride=8), :]
        theirs = wide_other[pl.ds(m, slots, stride=8), :]
        square = square + mine * mine + theirs * theirs
    mean = jnp.sum(square, axis=1, keepdims=True) * (1.0 / MODEL_WIDTH)
    factor = lax.rsqrt(mean + EPS)
    for m in range(8):
        for source, number in ((wide, 2 * m + core), (wide_other, 2 * m + 1 - core)):
            values = source[pl.ds(m, slots, stride=8), :]
            normed = values * factor * gains[:, tile_at(number)]
            rows_in[:, tile_at(number)] = normed.astype(BF16)
    x = rows_in[...]
    acts = []
    for place in (packed, away):
        both = dot32(x, place[:depth, :])
        pre = both[:, :width]
        acts.append((pre / (1.0 + jnp.exp(-pre)) * both[:, width:]).astype(BF16))
    for q in range(4):
        at = slice(q * width, (q + 1) * width)
        part = dot32(acts[0], down[at, :])
        part = part + dot32(acts[1], away[depth + q * width : depth + (q + 1) * width, :])
        for k in range(2):
            wide[pl.ds(2 * q + k, slots, stride=8), :] = part[:, k * LANES : (k + 1) * LANES]
    for p in range(peers):
        out[p] = wide[p * rows : (p + 1) * rows, :].astype(BF16)


def combine_body(returned, weights, side, out, wide):
    peers, rows, _ = returned.shape
    slots = peers * rows // 8
    tokens = side.shape[0] // 8
    for p in range(peers):
        wide[p * rows : (p + 1) * rows, :] = returned[p].astype(F32)
    for m in range(8):
        block = wide[pl.ds(m, slots, stride=8), :].astype(BF16)
        sums = dot32(weights[...], block)
        routed = sums[:tokens] + sums[tokens : 2 * tokens] + sums[2 * tokens :]
        at = slice(m * tokens, (m + 1) * tokens)
        out[m] = (routed + side[at, :]).astype(BF16)


def final_body(index, tiles, middle, out):
    total = tiles[0].astype(F32)
    for j in range(1, tiles.shape[0]):
        total = total + tiles[j].astype(F32)
    tokens = out.shape[0]
    start = pl.multiple_of(index[0] // 2 * tokens, tokens)
    out[...] = (middle[pl.ds(start, tokens), :].astype(F32) + total).astype(BF16)


def on_device(
    hidden,
    lengths,
    latent_cache,
    cache_rotary,
    attn_gain,
    w_query_nope,
    w_query_rope,
    latent_weight,
    w_rotary_key,
    latent_norm_gain,
    key_up_weight,
    value_up_weight,
    head_gain,
    w_output,
    ffn_gain,
    expert_ids,
    expert_weights,
    w_expert_gate,
    w_expert_up,
    w_expert_down,
    w_shared_gate,
    w_shared_up,
    w_shared_down,
    w_dense_up,
    w_dense_down,
    dense_gate,
):
    tp = lax.axis_size("tp")
    ep = lax.axis_size("ep")
    index = lax.axis_index("tp").astype(jnp.int32).reshape(1)
    tokens = hidden.shape[0]
    slots = ep * CAP
    places = latent_cache.shape[1]
    chips = tp // 2
    same_core = [list(range(core, tp, 2)) for core in range(2)]
    small = shape((tp, 8, LANES), F32)
    half = (chips * tokens, LANES)
    large = shape((ep, slots * chips // ep, LANES), BF16)
    wide = pltpu.VMEM((slots * chips, LANES), F32)

    payload, normed = call(
        query_body,
        (small, shape(hidden.shape, BF16)),
        (hidden, attn_gain, w_query_nope.T, w_query_rope.T, key_up_weight),
        hbm=range(5),
        leave=(0,),
    )
    queries = exchange(payload, "tp")

    inverse = 1.0 / 10000.0 ** (jnp.arange(HALF, dtype=F32) / HALF)
    angles = lengths.astype(F32)[:, None] * inverse[None, :]
    cos, sin = jnp.cos(angles), jnp.sin(angles)
    token, cache = call(
        new_token_body,
        (
            shape((1, LATENT_UNITS + LANES), F32),
            shape((places + places * ROPE // LATENT_UNITS, LATENT_UNITS), BF16),
        ),
        (
            index,
            normed,
            latent_weight,
            w_rotary_key.T,
            latent_norm_gain,
            cos,
            sin,
            latent_cache,
            cache_rotary,
        ),
        smem=(0,),
        hbm=(2, 3, 4, 5, 6),
        raw=(7, 8),
        scratch=(pltpu.SemaphoreType.DMA((1 + places // LATENT_UNITS,)),),
    )
    queries, token = together(queries, token)

    payload = call(
        attention_body,
        small,
        (lengths, queries, cache, token, cos, sin),
        smem=(0,),
        leave=(0,),
    )
    payload, later = together(payload, index)
    attended = exchange(payload, "tp")
    pack, combine = call(
        prepare_body,
        (
            shape((PLAIN_QUERY + 16, LATENT_UNITS + chips * LANES), BF16),
            shape((3 * tokens, slots), BF16),
        ),
        (later, expert_ids.T, expert_weights.T, value_up_weight.T, head_gain, w_output),
        smem=(0,),
        hbm=range(1, 6),
    )
    pack = core_swap(pack)
    attended, pack, combine = together(attended, pack, combine)

    payload = call(
        head_body,
        shape((chips,) + half, BF16),
        (index, attended, value_up_weight.T, head_gain, w_output, pack),
        smem=(0,),
        leave=(0,),
    )
    payload, later = together(payload, index)
    shares = exchange(payload, "tp", same_core)
    width = w_expert_gate.shape[2]
    packed, down = call(
        pack_body,
        (shape((MODEL_WIDTH + 4 * width, 2 * width), BF16), shape((4 * width, 2 * width), BF16)),
        (later, w_expert_gate, w_expert_up, w_expert_down),
        smem=(0,),
        raw=(1, 2, 3),
        scratch=(pltpu.SemaphoreType.DMA((2 + 2 * chips,)),),
    )
    away = core_swap(packed)
    shares, packed, down, away = together(shares, packed, down, away)

    middle, payload = call(
        middle_body,
        (shape(half, BF16), large),
        (index, shares, hidden, expert_ids.T),
        smem=(0,),
        scratch=(wide,),
        leave=(1,),
    )
    payload, later = together(payload, middle)
    arrived = exchange(payload, "ep")
    other = core_swap(later)
    arrived, other = together(arrived, other)
    payload = call(
        expert_body,
        large,
        (
            index,
            arrived,
            core_swap(arrived),
            ffn_gain,
            packed,
            down,
            away,
        ),
        smem=(0,),
        leave=(0,),
        scratch=(
            wide,
            wide,
            pltpu.VMEM((slots, MODEL_WIDTH), BF16),
            pltpu.VMEM((1, MODEL_WIDTH), F32),
        ),
    )
    payload, later, other = together(payload, later, other)
    returned = exchange(payload, "ep")
    side, away = call(
        side_body,
        (shape(half, F32), shape(half, F32)),
        (
            index,
            later,
            other,
            ffn_gain,
            w_shared_gate.T,
            w_shared_up.T,
            w_shared_down,
            w_dense_up,
            w_dense_down,
            dense_gate,
        ),
        smem=(0,),
        hbm=range(3, 10),
        leave=(1,),
    )
    away = core_swap(away)
    returned, side = together(returned, side + away)

    payload = call(
        combine_body,
        shape((chips, tokens, LANES), BF16),
        (returned, combine, side),
        scratch=(wide,),
    )
    parts = exchange(payload, "tp", same_core)
    return call(
        final_body, shape((tokens, LANES), BF16), (index, parts, middle), smem=(0,), leave=(0,)
    )


def solution(mesh):
    placed = (
        P("ep", None),
        P(("ep", "tp")),
        P(("ep", "tp"), None, None),
        P(("ep", "tp"), None, None),
        P(),
        P(None, "tp"),
        P(None, "tp"),
        P(),
        P(),
        P(),
        P("tp", None),
        P(None, "tp"),
        P("tp"),
        P("tp", None),
        P(),
        P("ep", None),
        P("ep", None),
        P("ep", None, "tp"),
        P("ep", None, "tp"),
        P("ep", "tp", None),
        P(None, "tp"),
        P(None, "tp"),
        P("tp", None),
        P(None, "tp"),
        P("tp", None),
        P(),
    )
    return jax.shard_map(
        on_device, mesh=mesh, in_specs=placed, out_specs=P("ep", "tp"), check_vma=False
    )
```

```python
import jax
import jax.numpy as jnp
from jax import lax
from jax.experimental import pallas as pl
from jax.experimental.pallas import tpu as pltpu
from jax.sharding import PartitionSpec as P

MODEL_WIDTH = 2048
PLAIN_QUERY = 64
ROPE = 32
HALF = 16
LATENT_UNITS = 512
CAP = 2
LANES = 128
F32 = jnp.float32
BF16 = jnp.bfloat16
EPS = 1e-06


def exchange(x, axis, groups=None):
    return lax.all_to_all(
        x, axis, split_axis=0, concat_axis=0, axis_index_groups=groups, tiled=True
    )


def core_swap(x):
    return lax.ppermute(x, "tp", [(i, i ^ 1) for i in range(lax.axis_size("tp"))])


def dot32(a, b):
    return jnp.dot(a, b, preferred_element_type=F32)


def dot_t(a, b):
    return lax.dot_general(a, b, (((1,), (1,)), ((), ())), preferred_element_type=F32)


def call(body, outs, args, smem=(), hbm=(), raw=(), scratch=(), leave=()):
    vmem = pl.BlockSpec(memory_space=pltpu.VMEM)
    kinds = {i: pl.BlockSpec(memory_space=pltpu.SMEM) for i in smem}
    kinds.update({i: pl.BlockSpec(memory_space=pl.ANY) for i in raw})
    free = set(smem) | set(hbm) | set(raw)
    scalars = set(smem)
    args = [
        x
        if i in scalars
        else pltpu.with_memory_space_constraint(x, pltpu.HBM if i in free else pltpu.VMEM)
        for i, x in enumerate(args)
    ]
    leaves, tree = jax.tree.flatten(outs)
    outs = tree.unflatten(
        (pltpu.HBM if i in leave else pltpu.VMEM)(o.shape, o.dtype) for i, o in enumerate(leaves)
    )
    return pl.pallas_call(
        body,
        out_shape=outs,
        in_specs=[kinds.get(i, vmem) for i in range(len(args))],
        out_specs=tree.unflatten(vmem for _ in leaves),
        scratch_shapes=list(scratch),
        compiler_params=pltpu.CompilerParams(vmem_limit_bytes=16 * 1024 * 1024),
    )(*args)


def together(*values):
    return lax.optimization_barrier(values)


def shape(dims, dtype):
    return jax.ShapeDtypeStruct(dims, dtype)


def row(gain):
    return gain[...].astype(F32).reshape(1, -1)


def query_body(*refs):
    sources, (out, normed_out, *held, sems) = refs[:5], refs[5:]
    copies = [
        pltpu.make_async_copy(source, place, sems.at[k])
        for k, (source, place) in enumerate(zip(sources, held))
    ]
    for copy in copies:
        copy.start()
    hidden, gain, w_nope, w_rope, key_up = held
    copies[0].wait()
    copies[1].wait()
    values = hidden[...].astype(F32)
    factor = lax.rsqrt(jnp.mean(values * values, axis=-1, keepdims=True) + EPS)
    normed = (values * factor * row(gain)).astype(BF16)
    normed_out[...] = normed
    for copy in copies[2:]:
        copy.wait()
    nope = dot_t(normed, w_nope[...]).astype(BF16)
    rope = dot_t(normed, w_rope[...]).astype(BF16).astype(F32)
    latent = dot32(nope, key_up[...]).astype(BF16).astype(F32)
    for s in range(LATENT_UNITS // LANES):
        out[:, s, :] = latent[:, s * LANES : (s + 1) * LANES]
    rows = out.shape[0]
    out[:, 4, :] = jnp.concatenate([rope, jnp.zeros((rows, LANES - ROPE), F32)], axis=1)
    for s in range(5, 8):
        out[:, s, :] = jnp.zeros((rows, LANES), F32)


def rotated(values, cos, sin):
    first, second = values[:, :HALF], values[:, HALF:ROPE]
    return jnp.concatenate([first * cos - second * sin, first * sin + second * cos], axis=1)


def new_token_body(
    index, normed, w_latent, w_key, gain, cos, sin, cache, rotary, out, cache_out, sems
):
    places, width = cache.shape[1:]
    copies = [pltpu.make_async_copy(cache.at[0], cache_out.at[pl.ds(0, places)], sems.at[0])]
    for k in range(rotary.shape[2] // width):
        source = rotary.at[0, :, pl.ds(k * width, width)]
        target = cache_out.at[pl.ds(places + k * ROPE, ROPE)]
        copies.append(pltpu.make_async_copy(source, target, sems.at[k + 1]))
    for copy in copies:
        copy.start()
    latent = dot32(normed[...], w_latent[...])
    key = dot_t(normed[...], w_key[...])
    rows = lax.broadcasted_iota(jnp.int32, (latent.shape[0], 1), 0)
    mine = rows == index[0]
    latent = jnp.sum(jnp.where(mine, latent, 0.0), axis=0, keepdims=True)
    key = jnp.sum(jnp.where(mine, key, 0.0), axis=0, keepdims=True)
    factor = lax.rsqrt(jnp.mean(latent * latent, axis=-1, keepdims=True) + EPS)
    out[:, :LATENT_UNITS] = (latent * factor * row(gain)).astype(BF16).astype(F32)
    key = rotated(key, cos[...], sin[...]).astype(BF16).astype(F32)
    out[:, LATENT_UNITS:] = jnp.concatenate([key, jnp.zeros((1, LANES - ROPE), F32)], axis=1)
    for copy in copies:
        copy.wait()


def attention_body(lengths, queries, caches, token, cos, sin, out):
    new_latent = token[:, :LATENT_UNITS]
    new_key = token[:, LATENT_UNITS : LATENT_UNITS + ROPE]
    parts = [queries[:, s, :] for s in range(LATENT_UNITS // LANES)]
    query = jnp.concatenate(parts, axis=1)
    rope = rotated(queries[:, 4, :], cos[...], sin[...]).astype(BF16)
    scale = (PLAIN_QUERY + ROPE) ** (-0.5)
    count = caches.shape[0] * LATENT_UNITS // (LATENT_UNITS + ROPE)
    cache = caches[:count, :]
    turned = [
        dot32(rope, caches[count + k * ROPE : count + (k + 1) * ROPE, :])
        for k in range(count // LATENT_UNITS)
    ]
    scores = dot_t(query.astype(BF16), cache) + jnp.concatenate(turned, axis=1)
    place = lax.broadcasted_iota(jnp.int32, scores.shape, 1)
    scores = jnp.where(place < lengths[0], scores * scale, -jnp.inf)
    own = jnp.sum(query * new_latent, axis=1, keepdims=True)
    own = own + jnp.sum(rope.astype(F32) * new_key, axis=1, keepdims=True)
    own = own * scale
    peak = jnp.maximum(jnp.max(scores, axis=1, keepdims=True), own)
    cache_exp = jnp.exp(scores - peak)
    own_exp = jnp.exp(own - peak)
    total = jnp.sum(cache_exp, axis=1, keepdims=True) + own_exp
    probs = (cache_exp / total).astype(BF16)
    own_probs = (own_exp / total).astype(BF16).astype(F32)
    mixed = dot32(probs, cache) + own_probs * new_latent
    mixed = mixed.astype(BF16).astype(F32)
    heads = mixed.shape[0]
    even = lax.broadcasted_iota(jnp.int32, mixed.shape, 0) % 2 == 0
    first = jnp.where(even, mixed, pltpu.roll(mixed, 1, 0))
    second = jnp.where(even, pltpu.roll(mixed, heads - 1, 0), mixed)
    count = LATENT_UNITS // LANES
    for s in range(count):
        tile = slice(s * LANES, (s + 1) * LANES)
        out[:, s, :] = first[:, tile]
        out[:, count + s, :] = second[:, tile]


def tile_at(number):
    return pl.ds(pl.multiple_of(number * LANES, LANES), LANES)


def slot_rows(ids_t, slots):
    top, tokens = ids_t.shape
    place = lax.broadcasted_iota(jnp.int32, (slots, tokens), 0)
    hits = [ids_t[k : k + 1, :] == place // CAP for k in range(top)]
    named = jnp.zeros((slots, tokens), F32)
    for hit in hits:
        named = named + jnp.where(hit, 1.0, 0.0)
    i = lax.broadcasted_iota(jnp.int32, (tokens, tokens), 0)
    j = lax.broadcasted_iota(jnp.int32, (tokens, tokens), 1)
    before = dot32(named.astype(BF16), jnp.where(i < j, 1.0, 0.0).astype(BF16))
    return jnp.where(before == (place % CAP).astype(F32), named, 0.0), hits


def prepare_body(index, ids_t, weights_t, value_up, gain, w_output, pack, combine):
    other = 1 - index[0] % 2
    rows = value_up.shape[0]
    pack[:rows, :LATENT_UNITS] = value_up[...]
    for m in range(8):
        at = LATENT_UNITS + m * LANES
        pack[:rows, at : at + LANES] = w_output[:, tile_at(2 * m + other)]
    wide_gain = jnp.concatenate([row(gain), jnp.zeros((1, LANES - rows), F32)], axis=1)
    pack[rows:, :] = jnp.zeros((16, pack.shape[1]), BF16)
    pack[rows:, :LANES] = jnp.broadcast_to(wide_gain, (16, LANES)).astype(BF16)

    tokens = ids_t.shape[1]
    taken, hits = slot_rows(ids_t, combine.shape[1])
    total = jnp.zeros(taken.shape, F32)
    for k, hit in enumerate(hits):
        total = total + jnp.where(hit, weights_t[k : k + 1, :], 0.0)
    total = jnp.where(taken > 0.0, total, 0.0)
    i = lax.broadcasted_iota(jnp.int32, (tokens, tokens), 0)
    j = lax.broadcasted_iota(jnp.int32, (tokens, tokens), 1)
    unit = jnp.where(i == j, 1.0, 0.0).astype(BF16)
    for p in range(3):
        part = total.astype(BF16)
        combine[p * tokens : (p + 1) * tokens, :] = dot_t(unit, part).astype(BF16)
        total = total - part.astype(F32)


def head_values(values, value_up, gains):
    head = dot_t(values.astype(BF16), value_up)
    factor = lax.rsqrt(jnp.mean(head * head, axis=-1, keepdims=True) + EPS)
    return (head * factor * gains).astype(BF16)


def head_body(index, attended, value_up, gain, w_output, pack, out):
    core = index[0] % 2
    count = LATENT_UNITS // LANES
    first = jnp.concatenate([attended[:, s, :] for s in range(count)], axis=1)
    second = jnp.concatenate([attended[:, count + s, :] for s in range(count)], axis=1)
    rows = value_up.shape[0]
    own = head_values(jnp.where(core == 0, first, second), value_up[...], row(gain))
    gains = pack[rows:, :LANES].astype(F32)[:1, :rows]
    other = head_values(
        jnp.where(core == 0, second, first), pack[:rows, :LATENT_UNITS], gains
    )
    tokens = own.shape[0]
    shares = dot32(other, pack[:rows, LATENT_UNITS:])
    for m in range(8):
        share = dot32(own, w_output[:, tile_at(2 * m + core)])
        share = (share + shares[:, m * LANES : (m + 1) * LANES]).astype(BF16)
        for p in range(out.shape[0]):
            out[p, m * tokens : (m + 1) * tokens, :] = share


def middle_body(index, shares, hidden, ids_t, middle_out, out, wide):
    core = index[0] % 2
    peers = shares.shape[0]
    tokens = hidden.shape[0]
    slots = wide.shape[0] // 8
    dispatch = slot_rows(ids_t, slots)[0].astype(BF16)
    for m in range(8):
        at = slice(m * tokens, (m + 1) * tokens)
        total = shares[0, at, :].astype(F32)
        for p in range(1, peers):
            total = total + shares[p, at, :].astype(F32)
        middle = (hidden[:, tile_at(2 * m + core)].astype(F32) + total).astype(BF16)
        middle_out[at, :] = middle
        wide[pl.ds(m, slots, stride=8), :] = dot32(dispatch, middle)
    rows = out.shape[1]
    for p in range(out.shape[0]):
        out[p] = wide[p * rows : (p + 1) * rows, :].astype(BF16)


def side_body(
    index, middle, other, gain, w_gate, w_up, w_shared_down, w_dense_up, w_dense_down, gate,
    own_out, other_out,
):
    core = index[0] % 2
    tokens = middle.shape[0] // 8
    tiles = []
    for j in range(16):
        at = slice(j // 2 * tokens, (j // 2 + 1) * tokens)
        mine, theirs = middle[at, :].astype(F32), other[at, :].astype(F32)
        tiles.append(jnp.where(core == j % 2, mine, theirs))
    values = jnp.concatenate(tiles, axis=1)
    factor = lax.rsqrt(jnp.mean(values * values, axis=-1, keepdims=True) + EPS)
    x = (values * factor * row(gain)).astype(BF16)
    pre = dot_t(x, w_gate[...])
    shared = (pre / (1.0 + jnp.exp(-pre)) * dot_t(x, w_up[...])).astype(BF16)
    dense = jax.nn.gelu(dot32(x, w_dense_up[...])).astype(BF16)
    logit = jnp.sum(x.astype(F32) * row(gate), axis=1, keepdims=True)
    mix = 1.0 / (1.0 + jnp.exp(-logit))
    side = dot32(shared, w_shared_down[...]) + mix * dot32(dense, w_dense_down[...])
    for m in range(8):
        at = slice(m * tokens, (m + 1) * tokens)
        low = side[:, 2 * m * LANES : (2 * m + 1) * LANES]
        high = side[:, (2 * m + 1) * LANES : (2 * m + 2) * LANES]
        own_out[at, :] = jnp.where(core == 0, low, high)
        other_out[at, :] = jnp.where(core == 0, high, low)


def pack_body(index, w_gate, w_up, w_down, packed, down, sems):
    core = index[0] % 2
    depth, width = w_gate.shape[1:]
    pairs = [
        (w.at[0], packed.at[pl.ds(0, depth), pl.ds(k * width, width)])
        for k, w in enumerate((w_gate, w_up))
    ]
    for place, base, parity in ((packed, depth, 1 - core), (down, 0, core)):
        for m in range(8):
            block = pl.ds(base + m // 2 * width, width), pl.ds(m % 2 * LANES, LANES)
            pairs.append((w_down.at[0, :, tile_at(2 * m + parity)], place.at[block]))
    copies = [pltpu.make_async_copy(*pair, sems.at[k]) for k, pair in enumerate(pairs)]
    for copy in copies:
        copy.start()
    for copy in copies:
        copy.wait()


def expert_body(
    index, arrived, other, gain, packed, down, away, out, wide, wide_other, rows_in, gains
):
    core = index[0] % 2
    depth = packed.shape[0] - down.shape[0]
    width = down.shape[0] // 4
    peers, rows, _ = arrived.shape
    slots = peers * rows // 8
    gains[...] = row(gain)
    for p in range(peers):
        at = slice(p * rows, (p + 1) * rows)
        wide[at, :] = arrived[p].astype(F32)
        wide_other[at, :] = other[p].astype(F32)
    square = jnp.zeros((slots, LANES), F32)
    for m in range(8):
        mine = wide[pl.ds(m, slots, stride=8), :]
        theirs = wide_other[pl.ds(m, slots, stride=8), :]
        square = square + mine * mine + theirs * theirs
    mean = jnp.sum(square, axis=1, keepdims=True) * (1.0 / MODEL_WIDTH)
    factor = lax.rsqrt(mean + EPS)
    for m in range(8):
        for source, number in ((wide, 2 * m + core), (wide_other, 2 * m + 1 - core)):
            values = source[pl.ds(m, slots, stride=8), :]
            normed = values * factor * gains[:, tile_at(number)]
            rows_in[:, tile_at(number)] = normed.astype(BF16)
    x = rows_in[...]
    acts = []
    for place in (packed, away):
        both = dot32(x, place[:depth, :])
        pre = both[:, :width]
        acts.append((pre / (1.0 + jnp.exp(-pre)) * both[:, width:]).astype(BF16))
    for q in range(4):
        at = slice(q * width, (q + 1) * width)
        part = dot32(acts[0], down[at, :])
        part = part + dot32(acts[1], away[depth + q * width : depth + (q + 1) * width, :])
        for k in range(2):
            wide[pl.ds(2 * q + k, slots, stride=8), :] = part[:, k * LANES : (k + 1) * LANES]
    for p in range(peers):
        out[p] = wide[p * rows : (p + 1) * rows, :].astype(BF16)


def combine_body(returned, weights, side, out, wide):
    peers, rows, _ = returned.shape
    slots = peers * rows // 8
    tokens = side.shape[0] // 8
    for p in range(peers):
        wide[p * rows : (p + 1) * rows, :] = returned[p].astype(F32)
    for m in range(8):
        block = wide[pl.ds(m, slots, stride=8), :].astype(BF16)
        sums = dot32(weights[...], block)
        routed = sums[:tokens] + sums[tokens : 2 * tokens] + sums[2 * tokens :]
        at = slice(m * tokens, (m + 1) * tokens)
        out[m] = (routed + side[at, :]).astype(BF16)


def final_body(index, tiles, middle, out):
    total = tiles[0].astype(F32)
    for j in range(1, tiles.shape[0]):
        total = total + tiles[j].astype(F32)
    tokens = out.shape[0]
    start = pl.multiple_of(index[0] // 2 * tokens, tokens)
    out[...] = (middle[pl.ds(start, tokens), :].astype(F32) + total).astype(BF16)


def on_device(
    hidden,
    lengths,
    latent_cache,
    cache_rotary,
    attn_gain,
    w_query_nope,
    w_query_rope,
    latent_weight,
    w_rotary_key,
    latent_norm_gain,
    key_up_weight,
    value_up_weight,
    head_gain,
    w_output,
    ffn_gain,
    expert_ids,
    expert_weights,
    w_expert_gate,
    w_expert_up,
    w_expert_down,
    w_shared_gate,
    w_shared_up,
    w_shared_down,
    w_dense_up,
    w_dense_down,
    dense_gate,
):
    tp = lax.axis_size("tp")
    ep = lax.axis_size("ep")
    index = lax.axis_index("tp").astype(jnp.int32).reshape(1)
    tokens = hidden.shape[0]
    slots = ep * CAP
    places = latent_cache.shape[1]
    chips = tp // 2
    same_core = [list(range(core, tp, 2)) for core in range(2)]
    small = shape((tp, 8, LANES), F32)
    half = (chips * tokens, LANES)
    large = shape((ep, slots * chips // ep, LANES), BF16)
    wide = pltpu.VMEM((slots * chips, LANES), F32)

    sources = (hidden, attn_gain, w_query_nope.T, w_query_rope.T, key_up_weight)
    payload, normed = call(
        query_body,
        (small, shape(hidden.shape, BF16)),
        sources,
        raw=range(5),
        leave=(0,),
        scratch=(
            *(pltpu.VMEM(x.shape, BF16) for x in sources),
            pltpu.SemaphoreType.DMA((len(sources),)),
        ),
    )
    queries = exchange(payload, "tp")

    inverse = 1.0 / 10000.0 ** (jnp.arange(HALF, dtype=F32) / HALF)
    angles = lengths.astype(F32)[:, None] * inverse[None, :]
    cos, sin = jnp.cos(angles), jnp.sin(angles)
    token, cache = call(
        new_token_body,
        (
            shape((1, LATENT_UNITS + LANES), F32),
            shape((places + places * ROPE // LATENT_UNITS, LATENT_UNITS), BF16),
        ),
        (
            index,
            normed,
            latent_weight,
            w_rotary_key.T,
            latent_norm_gain,
            cos,
            sin,
            latent_cache,
            cache_rotary,
        ),
        smem=(0,),
        hbm=(2, 3, 4, 5, 6),
        raw=(7, 8),
        scratch=(pltpu.SemaphoreType.DMA((1 + places // LATENT_UNITS,)),),
    )
    queries, token = together(queries, token)

    payload = call(
        attention_body,
        small,
        (lengths, queries, cache, token, cos, sin),
        smem=(0,),
        leave=(0,),
    )
    payload, later = together(payload, index)
    attended = exchange(payload, "tp")
    pack, combine = call(
        prepare_body,
        (
            shape((PLAIN_QUERY + 16, LATENT_UNITS + chips * LANES), BF16),
            shape((3 * tokens, slots), BF16),
        ),
        (later, expert_ids.T, expert_weights.T, value_up_weight.T, head_gain, w_output),
        smem=(0,),
        hbm=range(1, 6),
    )
    pack = core_swap(pack)
    attended, pack, combine = together(attended, pack, combine)

    payload = call(
        head_body,
        shape((chips,) + half, BF16),
        (index, attended, value_up_weight.T, head_gain, w_output, pack),
        smem=(0,),
    )
    shares = exchange(payload, "tp", same_core)

    middle, payload = call(
        middle_body,
        (shape(half, BF16), large),
        (index, shares, hidden, expert_ids.T),
        smem=(0,),
        scratch=(wide,),
        leave=(1,),
    )
    payload, later, when = together(payload, middle, index)
    arrived = exchange(payload, "ep")
    width = w_expert_gate.shape[2]
    packed, down = call(
        pack_body,
        (shape((MODEL_WIDTH + 4 * width, 2 * width), BF16), shape((4 * width, 2 * width), BF16)),
        (when, w_expert_gate, w_expert_up, w_expert_down),
        smem=(0,),
        raw=(1, 2, 3),
        scratch=(pltpu.SemaphoreType.DMA((2 + 2 * chips,)),),
    )
    away = core_swap(packed)
    arrived, packed, down, away = together(arrived, packed, down, away)
    payload = call(
        expert_body,
        large,
        (
            index,
            arrived,
            core_swap(arrived),
            ffn_gain,
            packed,
            down,
            away,
        ),
        smem=(0,),
        leave=(0,),
        scratch=(
            wide,
            wide,
            pltpu.VMEM((slots, MODEL_WIDTH), BF16),
            pltpu.VMEM((1, MODEL_WIDTH), F32),
        ),
    )
    payload, later = together(payload, later)
    returned = exchange(payload, "ep")
    other_half = core_swap(later)
    side, away = call(
        side_body,
        (shape(half, F32), shape(half, F32)),
        (
            index,
            later,
            other_half,
            ffn_gain,
            w_shared_gate.T,
            w_shared_up.T,
            w_shared_down,
            w_dense_up,
            w_dense_down,
            dense_gate,
        ),
        smem=(0,),
        hbm=range(3, 10),
        leave=(1,),
    )
    away = core_swap(away)
    returned, side = together(returned, side + away)

    payload = call(
        combine_body,
        shape((chips, tokens, LANES), BF16),
        (returned, combine, side),
        scratch=(wide,),
    )
    parts = exchange(payload, "tp", same_core)
    return call(
        final_body, shape((tokens, LANES), BF16), (index, parts, middle), smem=(0,), leave=(0,)
    )


def solution(mesh):
    placed = (
        P("ep", None),
        P(("ep", "tp")),
        P(("ep", "tp"), None, None),
        P(("ep", "tp"), None, None),
        P(),
        P(None, "tp"),
        P(None, "tp"),
        P(),
        P(),
        P(),
        P("tp", None),
        P(None, "tp"),
        P("tp"),
        P("tp", None),
        P(),
        P("ep", None),
        P("ep", None),
        P("ep", None, "tp"),
        P("ep", None, "tp"),
        P("ep", "tp", None),
        P(None, "tp"),
        P(None, "tp"),
        P("tp", None),
        P(None, "tp"),
        P("tp", None),
        P(),
    )
    return jax.shard_map(
        on_device, mesh=mesh, in_specs=placed, out_specs=P("ep", "tp"), check_vma=False
    )
```

```python
import jax
import jax.numpy as jnp
from jax import lax
from jax.experimental import pallas as pl
from jax.experimental.pallas import tpu as pltpu
from jax.sharding import PartitionSpec as P

MODEL_WIDTH = 2048
PLAIN_QUERY = 64
ROPE = 32
HALF = 16
LATENT_UNITS = 512
CAP = 2
LANES = 128
F32 = jnp.float32
BF16 = jnp.bfloat16
EPS = 1e-06


def exchange(x, axis, groups=None):
    return lax.all_to_all(
        x, axis, split_axis=0, concat_axis=0, axis_index_groups=groups, tiled=True
    )


def core_swap(x):
    return lax.ppermute(x, "tp", [(i, i ^ 1) for i in range(lax.axis_size("tp"))])


def dot32(a, b):
    return jnp.dot(a, b, preferred_element_type=F32)


def dot_t(a, b):
    return lax.dot_general(a, b, (((1,), (1,)), ((), ())), preferred_element_type=F32)


def call(body, outs, args, smem=(), hbm=(), raw=(), scratch=(), leave=()):
    vmem = pl.BlockSpec(memory_space=pltpu.VMEM)
    kinds = {i: pl.BlockSpec(memory_space=pltpu.SMEM) for i in smem}
    kinds.update({i: pl.BlockSpec(memory_space=pl.ANY) for i in raw})
    free = set(smem) | set(hbm) | set(raw)
    scalars = set(smem)
    args = [
        x
        if i in scalars
        else pltpu.with_memory_space_constraint(x, pltpu.HBM if i in free else pltpu.VMEM)
        for i, x in enumerate(args)
    ]
    leaves, tree = jax.tree.flatten(outs)
    outs = tree.unflatten(
        (pltpu.HBM if i in leave else pltpu.VMEM)(o.shape, o.dtype) for i, o in enumerate(leaves)
    )
    return pl.pallas_call(
        body,
        out_shape=outs,
        in_specs=[kinds.get(i, vmem) for i in range(len(args))],
        out_specs=tree.unflatten(vmem for _ in leaves),
        scratch_shapes=list(scratch),
        compiler_params=pltpu.CompilerParams(vmem_limit_bytes=16 * 1024 * 1024),
    )(*args)


def together(*values):
    return lax.optimization_barrier(values)


def shape(dims, dtype):
    return jax.ShapeDtypeStruct(dims, dtype)


def row(gain):
    return gain[...].astype(F32).reshape(1, -1)


def query_body(*refs):
    sources, (result, normed_out, *held, out, sems) = refs[:5], refs[5:]
    copies = [
        pltpu.make_async_copy(source, place, sems.at[k])
        for k, (source, place) in enumerate(zip(sources, held))
    ]
    for copy in copies:
        copy.start()
    hidden, gain, w_nope, w_rope, key_up = held
    copies[0].wait()
    copies[1].wait()
    values = hidden[...].astype(F32)
    factor = lax.rsqrt(jnp.mean(values * values, axis=-1, keepdims=True) + EPS)
    normed = (values * factor * row(gain)).astype(BF16)
    normed_out[...] = normed
    for copy in copies[2:]:
        copy.wait()
    nope = dot_t(normed, w_nope[...]).astype(BF16)
    rope = dot_t(normed, w_rope[...]).astype(BF16).astype(F32)
    latent = dot32(nope, key_up[...]).astype(BF16).astype(F32)
    for s in range(LATENT_UNITS // LANES):
        out[:, s, :] = latent[:, s * LANES : (s + 1) * LANES]
    rows = out.shape[0]
    out[:, 4, :] = jnp.concatenate([rope, jnp.zeros((rows, LANES - ROPE), F32)], axis=1)
    for s in range(5, 8):
        out[:, s, :] = jnp.zeros((rows, LANES), F32)
    result[...] = out[...].astype(BF16)


def rotated(values, cos, sin):
    first, second = values[:, :HALF], values[:, HALF:ROPE]
    return jnp.concatenate([first * cos - second * sin, first * sin + second * cos], axis=1)


def new_token_body(
    index, normed, w_latent, w_key, gain, cos, sin, cache, rotary, out, cache_out, sems
):
    places, width = cache.shape[1:]
    copies = [pltpu.make_async_copy(cache.at[0], cache_out.at[pl.ds(0, places)], sems.at[0])]
    for k in range(rotary.shape[2] // width):
        source = rotary.at[0, :, pl.ds(k * width, width)]
        target = cache_out.at[pl.ds(places + k * ROPE, ROPE)]
        copies.append(pltpu.make_async_copy(source, target, sems.at[k + 1]))
    for copy in copies:
        copy.start()
    latent = dot32(normed[...], w_latent[...])
    key = dot_t(normed[...], w_key[...])
    rows = lax.broadcasted_iota(jnp.int32, (latent.shape[0], 1), 0)
    mine = rows == index[0]
    latent = jnp.sum(jnp.where(mine, latent, 0.0), axis=0, keepdims=True)
    key = jnp.sum(jnp.where(mine, key, 0.0), axis=0, keepdims=True)
    factor = lax.rsqrt(jnp.mean(latent * latent, axis=-1, keepdims=True) + EPS)
    out[:, :LATENT_UNITS] = (latent * factor * row(gain)).astype(BF16).astype(F32)
    key = rotated(key, cos[...], sin[...]).astype(BF16).astype(F32)
    out[:, LATENT_UNITS:] = jnp.concatenate([key, jnp.zeros((1, LANES - ROPE), F32)], axis=1)
    for copy in copies:
        copy.wait()


def attention_body(lengths, arrived, caches, token, cos, sin, result, queries, out):
    queries[...] = arrived[...].astype(F32)
    new_latent = token[:, :LATENT_UNITS]
    new_key = token[:, LATENT_UNITS : LATENT_UNITS + ROPE]
    parts = [queries[:, s, :] for s in range(LATENT_UNITS // LANES)]
    query = jnp.concatenate(parts, axis=1)
    rope = rotated(queries[:, 4, :], cos[...], sin[...]).astype(BF16)
    scale = (PLAIN_QUERY + ROPE) ** (-0.5)
    count = caches.shape[0] * LATENT_UNITS // (LATENT_UNITS + ROPE)
    cache = caches[:count, :]
    turned = [
        dot32(rope, caches[count + k * ROPE : count + (k + 1) * ROPE, :])
        for k in range(count // LATENT_UNITS)
    ]
    scores = dot_t(query.astype(BF16), cache) + jnp.concatenate(turned, axis=1)
    place = lax.broadcasted_iota(jnp.int32, scores.shape, 1)
    scores = jnp.where(place < lengths[0], scores * scale, -jnp.inf)
    own = jnp.sum(query * new_latent, axis=1, keepdims=True)
    own = own + jnp.sum(rope.astype(F32) * new_key, axis=1, keepdims=True)
    own = own * scale
    peak = jnp.maximum(jnp.max(scores, axis=1, keepdims=True), own)
    cache_exp = jnp.exp(scores - peak)
    own_exp = jnp.exp(own - peak)
    total = jnp.sum(cache_exp, axis=1, keepdims=True) + own_exp
    probs = (cache_exp / total).astype(BF16)
    own_probs = (own_exp / total).astype(BF16).astype(F32)
    mixed = dot32(probs, cache) + own_probs * new_latent
    mixed = mixed.astype(BF16).astype(F32)
    heads = mixed.shape[0]
    even = lax.broadcasted_iota(jnp.int32, mixed.shape, 0) % 2 == 0
    first = jnp.where(even, mixed, pltpu.roll(mixed, 1, 0))
    second = jnp.where(even, pltpu.roll(mixed, heads - 1, 0), mixed)
    count = LATENT_UNITS // LANES
    for s in range(count):
        tile = slice(s * LANES, (s + 1) * LANES)
        out[:, s, :] = first[:, tile]
        out[:, count + s, :] = second[:, tile]
    result[...] = out[...].astype(BF16)


def tile_at(number):
    return pl.ds(pl.multiple_of(number * LANES, LANES), LANES)


def slot_rows(ids_t, slots):
    top, tokens = ids_t.shape
    place = lax.broadcasted_iota(jnp.int32, (slots, tokens), 0)
    hits = [ids_t[k : k + 1, :] == place // CAP for k in range(top)]
    named = jnp.zeros((slots, tokens), F32)
    for hit in hits:
        named = named + jnp.where(hit, 1.0, 0.0)
    i = lax.broadcasted_iota(jnp.int32, (tokens, tokens), 0)
    j = lax.broadcasted_iota(jnp.int32, (tokens, tokens), 1)
    before = dot32(named.astype(BF16), jnp.where(i < j, 1.0, 0.0).astype(BF16))
    return jnp.where(before == (place % CAP).astype(F32), named, 0.0), hits


def prepare_body(index, ids_t, weights_t, value_up, gain, w_output, pack, combine):
    other = 1 - index[0] % 2
    rows = value_up.shape[0]
    pack[:rows, :LATENT_UNITS] = value_up[...]
    for m in range(8):
        at = LATENT_UNITS + m * LANES
        pack[:rows, at : at + LANES] = w_output[:, tile_at(2 * m + other)]
    wide_gain = jnp.concatenate([row(gain), jnp.zeros((1, LANES - rows), F32)], axis=1)
    pack[rows:, :] = jnp.zeros((16, pack.shape[1]), BF16)
    pack[rows:, :LANES] = jnp.broadcast_to(wide_gain, (16, LANES)).astype(BF16)

    tokens = ids_t.shape[1]
    taken, hits = slot_rows(ids_t, combine.shape[1])
    total = jnp.zeros(taken.shape, F32)
    for k, hit in enumerate(hits):
        total = total + jnp.where(hit, weights_t[k : k + 1, :], 0.0)
    total = jnp.where(taken > 0.0, total, 0.0)
    i = lax.broadcasted_iota(jnp.int32, (tokens, tokens), 0)
    j = lax.broadcasted_iota(jnp.int32, (tokens, tokens), 1)
    unit = jnp.where(i == j, 1.0, 0.0).astype(BF16)
    for p in range(3):
        part = total.astype(BF16)
        combine[p * tokens : (p + 1) * tokens, :] = dot_t(unit, part).astype(BF16)
        total = total - part.astype(F32)


def head_values(values, value_up, gains):
    head = dot_t(values.astype(BF16), value_up)
    factor = lax.rsqrt(jnp.mean(head * head, axis=-1, keepdims=True) + EPS)
    return (head * factor * gains).astype(BF16)


def head_body(index, arrived, value_up, gain, w_output, pack, out, attended):
    attended[...] = arrived[...].astype(F32)
    core = index[0] % 2
    count = LATENT_UNITS // LANES
    first = jnp.concatenate([attended[:, s, :] for s in range(count)], axis=1)
    second = jnp.concatenate([attended[:, count + s, :] for s in range(count)], axis=1)
    rows = value_up.shape[0]
    own = head_values(jnp.where(core == 0, first, second), value_up[...], row(gain))
    gains = pack[rows:, :LANES].astype(F32)[:1, :rows]
    other = head_values(
        jnp.where(core == 0, second, first), pack[:rows, :LATENT_UNITS], gains
    )
    tokens = own.shape[0]
    shares = dot32(other, pack[:rows, LATENT_UNITS:])
    for m in range(8):
        share = dot32(own, w_output[:, tile_at(2 * m + core)])
        share = (share + shares[:, m * LANES : (m + 1) * LANES]).astype(BF16)
        for p in range(out.shape[0]):
            out[p, m * tokens : (m + 1) * tokens, :] = share


def middle_body(index, shares, hidden, ids_t, middle_out, out, wide):
    core = index[0] % 2
    peers = shares.shape[0]
    tokens = hidden.shape[0]
    slots = wide.shape[0] // 8
    dispatch = slot_rows(ids_t, slots)[0].astype(BF16)
    for m in range(8):
        at = slice(m * tokens, (m + 1) * tokens)
        total = shares[0, at, :].astype(F32)
        for p in range(1, peers):
            total = total + shares[p, at, :].astype(F32)
        middle = (hidden[:, tile_at(2 * m + core)].astype(F32) + total).astype(BF16)
        middle_out[at, :] = middle
        wide[pl.ds(m, slots, stride=8), :] = dot32(dispatch, middle)
    rows = out.shape[1]
    for p in range(out.shape[0]):
        out[p] = wide[p * rows : (p + 1) * rows, :].astype(BF16)


def side_body(
    index, middle, other, gain, w_gate, w_up, w_shared_down, w_dense_up, w_dense_down, gate,
    own_out, other_out,
):
    core = index[0] % 2
    tokens = middle.shape[0] // 8
    tiles = []
    for j in range(16):
        at = slice(j // 2 * tokens, (j // 2 + 1) * tokens)
        mine, theirs = middle[at, :].astype(F32), other[at, :].astype(F32)
        tiles.append(jnp.where(core == j % 2, mine, theirs))
    values = jnp.concatenate(tiles, axis=1)
    factor = lax.rsqrt(jnp.mean(values * values, axis=-1, keepdims=True) + EPS)
    x = (values * factor * row(gain)).astype(BF16)
    pre = dot_t(x, w_gate[...])
    shared = (pre / (1.0 + jnp.exp(-pre)) * dot_t(x, w_up[...])).astype(BF16)
    dense = jax.nn.gelu(dot32(x, w_dense_up[...])).astype(BF16)
    logit = jnp.sum(x.astype(F32) * row(gate), axis=1, keepdims=True)
    mix = 1.0 / (1.0 + jnp.exp(-logit))
    side = dot32(shared, w_shared_down[...]) + mix * dot32(dense, w_dense_down[...])
    for m in range(8):
        at = slice(m * tokens, (m + 1) * tokens)
        low = side[:, 2 * m * LANES : (2 * m + 1) * LANES]
        high = side[:, (2 * m + 1) * LANES : (2 * m + 2) * LANES]
        own_out[at, :] = jnp.where(core == 0, low, high)
        other_out[at, :] = jnp.where(core == 0, high, low)


def pack_body(index, w_gate, w_up, w_down, packed, down, sems):
    core = index[0] % 2
    depth, width = w_gate.shape[1:]
    pairs = [
        (w.at[0], packed.at[pl.ds(0, depth), pl.ds(k * width, width)])
        for k, w in enumerate((w_gate, w_up))
    ]
    for place, base, parity in ((packed, depth, 1 - core), (down, 0, core)):
        for m in range(8):
            block = pl.ds(base + m // 2 * width, width), pl.ds(m % 2 * LANES, LANES)
            pairs.append((w_down.at[0, :, tile_at(2 * m + parity)], place.at[block]))
    copies = [pltpu.make_async_copy(*pair, sems.at[k]) for k, pair in enumerate(pairs)]
    for copy in copies:
        copy.start()
    for copy in copies:
        copy.wait()


def expert_body(
    index, arrived, other, gain, packed, down, away, out, wide, wide_other, rows_in, gains
):
    core = index[0] % 2
    depth = packed.shape[0] - down.shape[0]
    width = down.shape[0] // 4
    peers, rows, _ = arrived.shape
    slots = peers * rows // 8
    gains[...] = row(gain)
    for p in range(peers):
        at = slice(p * rows, (p + 1) * rows)
        wide[at, :] = arrived[p].astype(F32)
        wide_other[at, :] = other[p].astype(F32)
    square = jnp.zeros((slots, LANES), F32)
    for m in range(8):
        mine = wide[pl.ds(m, slots, stride=8), :]
        theirs = wide_other[pl.ds(m, slots, stride=8), :]
        square = square + mine * mine + theirs * theirs
    mean = jnp.sum(square, axis=1, keepdims=True) * (1.0 / MODEL_WIDTH)
    factor = lax.rsqrt(mean + EPS)
    for m in range(8):
        for source, number in ((wide, 2 * m + core), (wide_other, 2 * m + 1 - core)):
            values = source[pl.ds(m, slots, stride=8), :]
            normed = values * factor * gains[:, tile_at(number)]
            rows_in[:, tile_at(number)] = normed.astype(BF16)
    x = rows_in[...]
    acts = []
    for place in (packed, away):
        both = dot32(x, place[:depth, :])
        pre = both[:, :width]
        acts.append((pre / (1.0 + jnp.exp(-pre)) * both[:, width:]).astype(BF16))
    for q in range(4):
        at = slice(q * width, (q + 1) * width)
        part = dot32(acts[0], down[at, :])
        part = part + dot32(acts[1], away[depth + q * width : depth + (q + 1) * width, :])
        for k in range(2):
            wide[pl.ds(2 * q + k, slots, stride=8), :] = part[:, k * LANES : (k + 1) * LANES]
    for p in range(peers):
        out[p] = wide[p * rows : (p + 1) * rows, :].astype(BF16)


def combine_body(returned, weights, side, out, wide):
    peers, rows, _ = returned.shape
    slots = peers * rows // 8
    tokens = side.shape[0] // 8
    for p in range(peers):
        wide[p * rows : (p + 1) * rows, :] = returned[p].astype(F32)
    for m in range(8):
        block = wide[pl.ds(m, slots, stride=8), :].astype(BF16)
        sums = dot32(weights[...], block)
        routed = sums[:tokens] + sums[tokens : 2 * tokens] + sums[2 * tokens :]
        at = slice(m * tokens, (m + 1) * tokens)
        out[m] = (routed + side[at, :]).astype(BF16)


def final_body(index, tiles, middle, out):
    total = tiles[0].astype(F32)
    for j in range(1, tiles.shape[0]):
        total = total + tiles[j].astype(F32)
    tokens = out.shape[0]
    start = pl.multiple_of(index[0] // 2 * tokens, tokens)
    out[...] = (middle[pl.ds(start, tokens), :].astype(F32) + total).astype(BF16)


def on_device(
    hidden,
    lengths,
    latent_cache,
    cache_rotary,
    attn_gain,
    w_query_nope,
    w_query_rope,
    latent_weight,
    w_rotary_key,
    latent_norm_gain,
    key_up_weight,
    value_up_weight,
    head_gain,
    w_output,
    ffn_gain,
    expert_ids,
    expert_weights,
    w_expert_gate,
    w_expert_up,
    w_expert_down,
    w_shared_gate,
    w_shared_up,
    w_shared_down,
    w_dense_up,
    w_dense_down,
    dense_gate,
):
    tp = lax.axis_size("tp")
    ep = lax.axis_size("ep")
    index = lax.axis_index("tp").astype(jnp.int32).reshape(1)
    tokens = hidden.shape[0]
    slots = ep * CAP
    places = latent_cache.shape[1]
    chips = tp // 2
    same_core = [list(range(core, tp, 2)) for core in range(2)]
    small = shape((tp, 8, LANES), BF16)
    spread = pltpu.VMEM((tp, 8, LANES), F32)
    half = (chips * tokens, LANES)
    large = shape((ep, slots * chips // ep, LANES), BF16)
    wide = pltpu.VMEM((slots * chips, LANES), F32)

    sources = (hidden, attn_gain, w_query_nope.T, w_query_rope.T, key_up_weight)
    payload, normed = call(
        query_body,
        (small, shape(hidden.shape, BF16)),
        sources,
        raw=range(5),
        leave=(0,),
        scratch=(
            *(pltpu.VMEM(x.shape, BF16) for x in sources),
            spread,
            pltpu.SemaphoreType.DMA((len(sources),)),
        ),
    )
    queries = exchange(payload, "tp")

    inverse = 1.0 / 10000.0 ** (jnp.arange(HALF, dtype=F32) / HALF)
    angles = lengths.astype(F32)[:, None] * inverse[None, :]
    cos, sin = jnp.cos(angles), jnp.sin(angles)
    token, cache = call(
        new_token_body,
        (
            shape((1, LATENT_UNITS + LANES), F32),
            shape((places + places * ROPE // LATENT_UNITS, LATENT_UNITS), BF16),
        ),
        (
            index,
            normed,
            latent_weight,
            w_rotary_key.T,
            latent_norm_gain,
            cos,
            sin,
            latent_cache,
            cache_rotary,
        ),
        smem=(0,),
        hbm=(2, 3, 4, 5, 6),
        raw=(7, 8),
        scratch=(pltpu.SemaphoreType.DMA((1 + places // LATENT_UNITS,)),),
    )
    queries, token = together(queries, token)

    payload = call(
        attention_body,
        small,
        (lengths, queries, cache, token, cos, sin),
        smem=(0,),
        leave=(0,),
        scratch=(spread, spread),
    )
    payload, later = together(payload, index)
    attended = exchange(payload, "tp")
    pack, combine = call(
        prepare_body,
        (
            shape((PLAIN_QUERY + 16, LATENT_UNITS + chips * LANES), BF16),
            shape((3 * tokens, slots), BF16),
        ),
        (later, expert_ids.T, expert_weights.T, value_up_weight.T, head_gain, w_output),
        smem=(0,),
        hbm=range(1, 6),
    )
    pack = core_swap(pack)
    attended, pack, combine = together(attended, pack, combine)

    payload = call(
        head_body,
        shape((chips,) + half, BF16),
        (index, attended, value_up_weight.T, head_gain, w_output, pack),
        smem=(0,),
        scratch=(spread,),
    )
    shares = exchange(payload, "tp", same_core)

    middle, payload = call(
        middle_body,
        (shape(half, BF16), large),
        (index, shares, hidden, expert_ids.T),
        smem=(0,),
        scratch=(wide,),
        leave=(1,),
    )
    payload, later, when = together(payload, middle, index)
    arrived = exchange(payload, "ep")
    width = w_expert_gate.shape[2]
    packed, down = call(
        pack_body,
        (shape((MODEL_WIDTH + 4 * width, 2 * width), BF16), shape((4 * width, 2 * width), BF16)),
        (when, w_expert_gate, w_expert_up, w_expert_down),
        smem=(0,),
        raw=(1, 2, 3),
        scratch=(pltpu.SemaphoreType.DMA((2 + 2 * chips,)),),
    )
    away = core_swap(packed)
    arrived, packed, down, away = together(arrived, packed, down, away)
    payload = call(
        expert_body,
        large,
        (
            index,
            arrived,
            core_swap(arrived),
            ffn_gain,
            packed,
            down,
            away,
        ),
        smem=(0,),
        leave=(0,),
        scratch=(
            wide,
            wide,
            pltpu.VMEM((slots, MODEL_WIDTH), BF16),
            pltpu.VMEM((1, MODEL_WIDTH), F32),
        ),
    )
    payload, later = together(payload, later)
    returned = exchange(payload, "ep")
    other_half = core_swap(later)
    side, away = call(
        side_body,
        (shape(half, F32), shape(half, F32)),
        (
            index,
            later,
            other_half,
            ffn_gain,
            w_shared_gate.T,
            w_shared_up.T,
            w_shared_down,
            w_dense_up,
            w_dense_down,
            dense_gate,
        ),
        smem=(0,),
        hbm=range(3, 10),
        leave=(1,),
    )
    away = core_swap(away)
    returned, side = together(returned, side + away)

    payload = call(
        combine_body,
        shape((chips, tokens, LANES), BF16),
        (returned, combine, side),
        scratch=(wide,),
    )
    parts = exchange(payload, "tp", same_core)
    return call(
        final_body, shape((tokens, LANES), BF16), (index, parts, middle), smem=(0,), leave=(0,)
    )


def solution(mesh):
    placed = (
        P("ep", None),
        P(("ep", "tp")),
        P(("ep", "tp"), None, None),
        P(("ep", "tp"), None, None),
        P(),
        P(None, "tp"),
        P(None, "tp"),
        P(),
        P(),
        P(),
        P("tp", None),
        P(None, "tp"),
        P("tp"),
        P("tp", None),
        P(),
        P("ep", None),
        P("ep", None),
        P("ep", None, "tp"),
        P("ep", None, "tp"),
        P("ep", "tp", None),
        P(None, "tp"),
        P(None, "tp"),
        P("tp", None),
        P(None, "tp"),
        P("tp", None),
        P(),
    )
    return jax.shard_map(
        on_device, mesh=mesh, in_specs=placed, out_specs=P("ep", "tp"), check_vma=False
    )
```

```python
import jax
import jax.numpy as jnp
from jax import lax
from jax.experimental import pallas as pl
from jax.experimental.pallas import tpu as pltpu
from jax.sharding import PartitionSpec as P

MODEL_WIDTH = 2048
PLAIN_QUERY = 64
ROPE = 32
HALF = 16
LATENT_UNITS = 512
CAP = 2
LANES = 128
F32 = jnp.float32
BF16 = jnp.bfloat16
EPS = 1e-06


def exchange(x, axis, groups=None):
    return lax.all_to_all(
        x, axis, split_axis=0, concat_axis=0, axis_index_groups=groups, tiled=True
    )


def core_swap(x):
    return lax.ppermute(x, "tp", [(i, i ^ 1) for i in range(lax.axis_size("tp"))])


def dot32(a, b):
    return jnp.dot(a, b, preferred_element_type=F32)


def dot_t(a, b):
    return lax.dot_general(a, b, (((1,), (1,)), ((), ())), preferred_element_type=F32)


def call(body, outs, args, smem=(), hbm=(), raw=(), scratch=(), leave=()):
    vmem = pl.BlockSpec(memory_space=pltpu.VMEM)
    kinds = {i: pl.BlockSpec(memory_space=pltpu.SMEM) for i in smem}
    kinds.update({i: pl.BlockSpec(memory_space=pl.ANY) for i in raw})
    free = set(smem) | set(hbm) | set(raw)
    scalars = set(smem)
    args = [
        x
        if i in scalars
        else pltpu.with_memory_space_constraint(x, pltpu.HBM if i in free else pltpu.VMEM)
        for i, x in enumerate(args)
    ]
    leaves, tree = jax.tree.flatten(outs)
    outs = tree.unflatten(
        (pltpu.HBM if i in leave else pltpu.VMEM)(o.shape, o.dtype) for i, o in enumerate(leaves)
    )
    return pl.pallas_call(
        body,
        out_shape=outs,
        in_specs=[kinds.get(i, vmem) for i in range(len(args))],
        out_specs=tree.unflatten(vmem for _ in leaves),
        scratch_shapes=list(scratch),
        compiler_params=pltpu.CompilerParams(vmem_limit_bytes=16 * 1024 * 1024),
    )(*args)


def together(*values):
    return lax.optimization_barrier(values)


def shape(dims, dtype):
    return jax.ShapeDtypeStruct(dims, dtype)


def row(gain):
    return gain[...].astype(F32).reshape(1, -1)


def query_body(*refs):
    sources, (result, normed_out, *held, out, sems) = refs[:5], refs[5:]
    copies = [
        pltpu.make_async_copy(source, place, sems.at[k])
        for k, (source, place) in enumerate(zip(sources, held))
    ]
    for copy in copies:
        copy.start()
    hidden, gain, w_nope, w_rope, key_up = held
    copies[0].wait()
    copies[1].wait()
    values = hidden[...].astype(F32)
    factor = lax.rsqrt(jnp.mean(values * values, axis=-1, keepdims=True) + EPS)
    normed = (values * factor * row(gain)).astype(BF16)
    normed_out[...] = normed
    for copy in copies[2:]:
        copy.wait()
    nope = dot_t(normed, w_nope[...]).astype(BF16)
    rope = dot_t(normed, w_rope[...]).astype(BF16).astype(F32)
    latent = dot32(nope, key_up[...]).astype(BF16).astype(F32)
    for s in range(LATENT_UNITS // LANES):
        out[:, s, :] = latent[:, s * LANES : (s + 1) * LANES]
    rows = out.shape[0]
    out[:, 4, :] = jnp.concatenate([rope, jnp.zeros((rows, LANES - ROPE), F32)], axis=1)
    for s in range(5, 8):
        out[:, s, :] = jnp.zeros((rows, LANES), F32)
    result[...] = out[...].astype(BF16)


def rotated(values, cos, sin):
    first, second = values[:, :HALF], values[:, HALF:ROPE]
    return jnp.concatenate([first * cos - second * sin, first * sin + second * cos], axis=1)


def new_token_body(
    index, normed, w_latent, w_key, gain, cos, sin, cache, rotary, out, cache_out, sems
):
    places, width = cache.shape[1:]
    copies = [pltpu.make_async_copy(cache.at[0], cache_out.at[pl.ds(0, places)], sems.at[0])]
    for k in range(rotary.shape[2] // width):
        source = rotary.at[0, :, pl.ds(k * width, width)]
        target = cache_out.at[pl.ds(places + k * ROPE, ROPE)]
        copies.append(pltpu.make_async_copy(source, target, sems.at[k + 1]))
    for copy in copies:
        copy.start()
    latent = dot32(normed[...], w_latent[...])
    key = dot_t(normed[...], w_key[...])
    rows = lax.broadcasted_iota(jnp.int32, (latent.shape[0], 1), 0)
    mine = rows == index[0]
    latent = jnp.sum(jnp.where(mine, latent, 0.0), axis=0, keepdims=True)
    key = jnp.sum(jnp.where(mine, key, 0.0), axis=0, keepdims=True)
    factor = lax.rsqrt(jnp.mean(latent * latent, axis=-1, keepdims=True) + EPS)
    out[:, :LATENT_UNITS] = (latent * factor * row(gain)).astype(BF16).astype(F32)
    key = rotated(key, cos[...], sin[...]).astype(BF16).astype(F32)
    out[:, LATENT_UNITS:] = jnp.concatenate([key, jnp.zeros((1, LANES - ROPE), F32)], axis=1)
    for copy in copies:
        copy.wait()


def attention_body(lengths, arrived, caches, token, cos, sin, result, queries, out):
    queries[...] = arrived[...].astype(F32)
    new_latent = token[:, :LATENT_UNITS]
    new_key = token[:, LATENT_UNITS : LATENT_UNITS + ROPE]
    parts = [queries[:, s, :] for s in range(LATENT_UNITS // LANES)]
    query = jnp.concatenate(parts, axis=1)
    rope = rotated(queries[:, 4, :], cos[...], sin[...]).astype(BF16)
    scale = (PLAIN_QUERY + ROPE) ** (-0.5)
    count = caches.shape[0] * LATENT_UNITS // (LATENT_UNITS + ROPE)
    cache = caches[:count, :]
    turned = [
        dot32(rope, caches[count + k * ROPE : count + (k + 1) * ROPE, :])
        for k in range(count // LATENT_UNITS)
    ]
    scores = dot_t(query.astype(BF16), cache) + jnp.concatenate(turned, axis=1)
    place = lax.broadcasted_iota(jnp.int32, scores.shape, 1)
    scores = jnp.where(place < lengths[0], scores * scale, -jnp.inf)
    own = jnp.sum(query * new_latent, axis=1, keepdims=True)
    own = own + jnp.sum(rope.astype(F32) * new_key, axis=1, keepdims=True)
    own = own * scale
    peak = jnp.maximum(jnp.max(scores, axis=1, keepdims=True), own)
    cache_exp = jnp.exp(scores - peak)
    own_exp = jnp.exp(own - peak)
    total = jnp.sum(cache_exp, axis=1, keepdims=True) + own_exp
    probs = (cache_exp / total).astype(BF16)
    own_probs = (own_exp / total).astype(BF16).astype(F32)
    mixed = dot32(probs, cache) + own_probs * new_latent
    mixed = mixed.astype(BF16).astype(F32)
    heads = mixed.shape[0]
    even = lax.broadcasted_iota(jnp.int32, mixed.shape, 0) % 2 == 0
    first = jnp.where(even, mixed, pltpu.roll(mixed, 1, 0))
    second = jnp.where(even, pltpu.roll(mixed, heads - 1, 0), mixed)
    count = LATENT_UNITS // LANES
    for s in range(count):
        tile = slice(s * LANES, (s + 1) * LANES)
        out[:, s, :] = first[:, tile]
        out[:, count + s, :] = second[:, tile]
    result[...] = out[...].astype(BF16)


def tile_at(number):
    return pl.ds(pl.multiple_of(number * LANES, LANES), LANES)


def slot_rows(ids_t, slots):
    top, tokens = ids_t.shape
    place = lax.broadcasted_iota(jnp.int32, (slots, tokens), 0)
    hits = [ids_t[k : k + 1, :] == place // CAP for k in range(top)]
    named = jnp.zeros((slots, tokens), F32)
    for hit in hits:
        named = named + jnp.where(hit, 1.0, 0.0)
    i = lax.broadcasted_iota(jnp.int32, (tokens, tokens), 0)
    j = lax.broadcasted_iota(jnp.int32, (tokens, tokens), 1)
    before = dot32(named.astype(BF16), jnp.where(i < j, 1.0, 0.0).astype(BF16))
    return jnp.where(before == (place % CAP).astype(F32), named, 0.0), hits


def prepare_body(index, ids_t, weights_t, value_up, gain, w_output, pack, combine):
    other = 1 - index[0] % 2
    rows = value_up.shape[0]
    pack[:rows, :LATENT_UNITS] = value_up[...]
    for m in range(8):
        at = LATENT_UNITS + m * LANES
        pack[:rows, at : at + LANES] = w_output[:, tile_at(2 * m + other)]
    wide_gain = jnp.concatenate([row(gain), jnp.zeros((1, LANES - rows), F32)], axis=1)
    pack[rows:, :] = jnp.zeros((16, pack.shape[1]), BF16)
    pack[rows:, :LANES] = jnp.broadcast_to(wide_gain, (16, LANES)).astype(BF16)

    tokens = ids_t.shape[1]
    taken, hits = slot_rows(ids_t, combine.shape[1])
    total = jnp.zeros(taken.shape, F32)
    for k, hit in enumerate(hits):
        total = total + jnp.where(hit, weights_t[k : k + 1, :], 0.0)
    total = jnp.where(taken > 0.0, total, 0.0)
    i = lax.broadcasted_iota(jnp.int32, (tokens, tokens), 0)
    j = lax.broadcasted_iota(jnp.int32, (tokens, tokens), 1)
    unit = jnp.where(i == j, 1.0, 0.0).astype(BF16)
    for p in range(3):
        part = total.astype(BF16)
        combine[p * tokens : (p + 1) * tokens, :] = dot_t(unit, part).astype(BF16)
        total = total - part.astype(F32)


def head_values(values, value_up, gains):
    head = dot_t(values.astype(BF16), value_up)
    factor = lax.rsqrt(jnp.mean(head * head, axis=-1, keepdims=True) + EPS)
    return (head * factor * gains).astype(BF16)


def head_body(index, arrived, value_up, gain, w_output, pack, out, attended):
    attended[...] = arrived[...].astype(F32)
    core = index[0] % 2
    count = LATENT_UNITS // LANES
    first = jnp.concatenate([attended[:, s, :] for s in range(count)], axis=1)
    second = jnp.concatenate([attended[:, count + s, :] for s in range(count)], axis=1)
    rows = value_up.shape[0]
    own = head_values(jnp.where(core == 0, first, second), value_up[...], row(gain))
    gains = pack[rows:, :LANES].astype(F32)[:1, :rows]
    other = head_values(
        jnp.where(core == 0, second, first), pack[:rows, :LATENT_UNITS], gains
    )
    tokens = own.shape[0]
    shares = dot32(other, pack[:rows, LATENT_UNITS:])
    for m in range(8):
        share = dot32(own, w_output[:, tile_at(2 * m + core)])
        share = (share + shares[:, m * LANES : (m + 1) * LANES]).astype(BF16)
        for p in range(out.shape[0]):
            out[p, m * tokens : (m + 1) * tokens, :] = share


def middle_body(index, shares, hidden, ids_t, middle_out, out, wide):
    core = index[0] % 2
    peers = shares.shape[0]
    tokens = hidden.shape[0]
    slots = wide.shape[0] // 8
    dispatch = slot_rows(ids_t, slots)[0].astype(BF16)
    for m in range(8):
        at = slice(m * tokens, (m + 1) * tokens)
        total = shares[0, at, :].astype(F32)
        for p in range(1, peers):
            total = total + shares[p, at, :].astype(F32)
        middle = (hidden[:, tile_at(2 * m + core)].astype(F32) + total).astype(BF16)
        middle_out[at, :] = middle
        wide[pl.ds(m, slots, stride=8), :] = dot32(dispatch, middle)
    rows = out.shape[1]
    for p in range(out.shape[0]):
        out[p] = wide[p * rows : (p + 1) * rows, :].astype(BF16)


def side_body(index, middle, other, *refs):
    sources, (own_out, other_out, *held, sems) = refs[:7], refs[7:]
    copies = [
        pltpu.make_async_copy(source, place, sems.at[k])
        for k, (source, place) in enumerate(zip(sources, held))
    ]
    for copy in copies:
        copy.start()
    gain, gate, w_gate, w_up, w_dense_up, w_shared_down, w_dense_down = held
    core = index[0] % 2
    tokens = middle.shape[0] // 8
    tiles = []
    for j in range(16):
        at = slice(j // 2 * tokens, (j // 2 + 1) * tokens)
        mine, theirs = middle[at, :].astype(F32), other[at, :].astype(F32)
        tiles.append(jnp.where(core == j % 2, mine, theirs))
    values = jnp.concatenate(tiles, axis=1)
    factor = lax.rsqrt(jnp.mean(values * values, axis=-1, keepdims=True) + EPS)
    copies[0].wait()
    x = (values * factor * row(gain)).astype(BF16)
    for copy in copies[1:]:
        copy.wait()
    pre = dot_t(x, w_gate[...])
    shared = (pre / (1.0 + jnp.exp(-pre)) * dot_t(x, w_up[...])).astype(BF16)
    dense = jax.nn.gelu(dot32(x, w_dense_up[...])).astype(BF16)
    logit = jnp.sum(x.astype(F32) * row(gate), axis=1, keepdims=True)
    mix = 1.0 / (1.0 + jnp.exp(-logit))
    side = dot32(shared, w_shared_down[...]) + mix * dot32(dense, w_dense_down[...])
    for m in range(8):
        at = slice(m * tokens, (m + 1) * tokens)
        low = side[:, 2 * m * LANES : (2 * m + 1) * LANES]
        high = side[:, (2 * m + 1) * LANES : (2 * m + 2) * LANES]
        own_out[at, :] = jnp.where(core == 0, low, high)
        other_out[at, :] = jnp.where(core == 0, high, low)


def pack_body(index, w_gate, w_up, w_down, packed, down, sems):
    core = index[0] % 2
    depth, width = w_gate.shape[1:]
    pairs = [
        (w.at[0], packed.at[pl.ds(0, depth), pl.ds(k * width, width)])
        for k, w in enumerate((w_gate, w_up))
    ]
    for place, base, parity in ((packed, depth, 1 - core), (down, 0, core)):
        for m in range(8):
            block = pl.ds(base + m // 2 * width, width), pl.ds(m % 2 * LANES, LANES)
            pairs.append((w_down.at[0, :, tile_at(2 * m + parity)], place.at[block]))
    copies = [pltpu.make_async_copy(*pair, sems.at[k]) for k, pair in enumerate(pairs)]
    for copy in copies:
        copy.start()
    for copy in copies:
        copy.wait()


def expert_body(
    index, arrived, other, gain, packed, down, away, out, wide, wide_other, rows_in, gains
):
    core = index[0] % 2
    depth = packed.shape[0] - down.shape[0]
    width = down.shape[0] // 4
    peers, rows, _ = arrived.shape
    slots = peers * rows // 8
    gains[...] = row(gain)
    for p in range(peers):
        at = slice(p * rows, (p + 1) * rows)
        wide[at, :] = arrived[p].astype(F32)
        wide_other[at, :] = other[p].astype(F32)
    square = jnp.zeros((slots, LANES), F32)
    for m in range(8):
        mine = wide[pl.ds(m, slots, stride=8), :]
        theirs = wide_other[pl.ds(m, slots, stride=8), :]
        square = square + mine * mine + theirs * theirs
    mean = jnp.sum(square, axis=1, keepdims=True) * (1.0 / MODEL_WIDTH)
    factor = lax.rsqrt(mean + EPS)
    for m in range(8):
        for source, number in ((wide, 2 * m + core), (wide_other, 2 * m + 1 - core)):
            values = source[pl.ds(m, slots, stride=8), :]
            normed = values * factor * gains[:, tile_at(number)]
            rows_in[:, tile_at(number)] = normed.astype(BF16)
    x = rows_in[...]
    acts = []
    for place in (packed, away):
        both = dot32(x, place[:depth, :])
        pre = both[:, :width]
        acts.append((pre / (1.0 + jnp.exp(-pre)) * both[:, width:]).astype(BF16))
    for q in range(4):
        at = slice(q * width, (q + 1) * width)
        part = dot32(acts[0], down[at, :])
        part = part + dot32(acts[1], away[depth + q * width : depth + (q + 1) * width, :])
        for k in range(2):
            wide[pl.ds(2 * q + k, slots, stride=8), :] = part[:, k * LANES : (k + 1) * LANES]
    for p in range(peers):
        out[p] = wide[p * rows : (p + 1) * rows, :].astype(BF16)


def combine_body(returned, weights, side, out, wide):
    peers, rows, _ = returned.shape
    slots = peers * rows // 8
    tokens = side.shape[0] // 8
    for p in range(peers):
        wide[p * rows : (p + 1) * rows, :] = returned[p].astype(F32)
    for m in range(8):
        block = wide[pl.ds(m, slots, stride=8), :].astype(BF16)
        sums = dot32(weights[...], block)
        routed = sums[:tokens] + sums[tokens : 2 * tokens] + sums[2 * tokens :]
        at = slice(m * tokens, (m + 1) * tokens)
        out[m] = (routed + side[at, :]).astype(BF16)


def final_body(index, tiles, middle, out):
    total = tiles[0].astype(F32)
    for j in range(1, tiles.shape[0]):
        total = total + tiles[j].astype(F32)
    tokens = out.shape[0]
    start = pl.multiple_of(index[0] // 2 * tokens, tokens)
    out[...] = (middle[pl.ds(start, tokens), :].astype(F32) + total).astype(BF16)


def on_device(
    hidden,
    lengths,
    latent_cache,
    cache_rotary,
    attn_gain,
    w_query_nope,
    w_query_rope,
    latent_weight,
    w_rotary_key,
    latent_norm_gain,
    key_up_weight,
    value_up_weight,
    head_gain,
    w_output,
    ffn_gain,
    expert_ids,
    expert_weights,
    w_expert_gate,
    w_expert_up,
    w_expert_down,
    w_shared_gate,
    w_shared_up,
    w_shared_down,
    w_dense_up,
    w_dense_down,
    dense_gate,
):
    tp = lax.axis_size("tp")
    ep = lax.axis_size("ep")
    index = lax.axis_index("tp").astype(jnp.int32).reshape(1)
    tokens = hidden.shape[0]
    slots = ep * CAP
    places = latent_cache.shape[1]
    chips = tp // 2
    same_core = [list(range(core, tp, 2)) for core in range(2)]
    small = shape((tp, 8, LANES), BF16)
    spread = pltpu.VMEM((tp, 8, LANES), F32)
    half = (chips * tokens, LANES)
    large = shape((ep, slots * chips // ep, LANES), BF16)
    wide = pltpu.VMEM((slots * chips, LANES), F32)

    sources = (hidden, attn_gain, w_query_nope.T, w_query_rope.T, key_up_weight)
    payload, normed = call(
        query_body,
        (small, shape(hidden.shape, BF16)),
        sources,
        raw=range(5),
        leave=(0,),
        scratch=(
            *(pltpu.VMEM(x.shape, BF16) for x in sources),
            spread,
            pltpu.SemaphoreType.DMA((len(sources),)),
        ),
    )
    queries = exchange(payload, "tp")

    inverse = 1.0 / 10000.0 ** (jnp.arange(HALF, dtype=F32) / HALF)
    angles = lengths.astype(F32)[:, None] * inverse[None, :]
    cos, sin = jnp.cos(angles), jnp.sin(angles)
    token, cache = call(
        new_token_body,
        (
            shape((1, LATENT_UNITS + LANES), F32),
            shape((places + places * ROPE // LATENT_UNITS, LATENT_UNITS), BF16),
        ),
        (
            index,
            normed,
            latent_weight,
            w_rotary_key.T,
            latent_norm_gain,
            cos,
            sin,
            latent_cache,
            cache_rotary,
        ),
        smem=(0,),
        hbm=(2, 3, 4, 5, 6),
        raw=(7, 8),
        scratch=(pltpu.SemaphoreType.DMA((1 + places // LATENT_UNITS,)),),
    )
    queries, token = together(queries, token)

    payload = call(
        attention_body,
        small,
        (lengths, queries, cache, token, cos, sin),
        smem=(0,),
        leave=(0,),
        scratch=(spread, spread),
    )
    payload, later = together(payload, index)
    attended = exchange(payload, "tp")
    pack, combine = call(
        prepare_body,
        (
            shape((PLAIN_QUERY + 16, LATENT_UNITS + chips * LANES), BF16),
            shape((3 * tokens, slots), BF16),
        ),
        (later, expert_ids.T, expert_weights.T, value_up_weight.T, head_gain, w_output),
        smem=(0,),
        hbm=range(1, 6),
    )
    pack = core_swap(pack)
    attended, pack, combine = together(attended, pack, combine)

    payload = call(
        head_body,
        shape((chips,) + half, BF16),
        (index, attended, value_up_weight.T, head_gain, w_output, pack),
        smem=(0,),
        scratch=(spread,),
    )
    shares = exchange(payload, "tp", same_core)

    middle, payload = call(
        middle_body,
        (shape(half, BF16), large),
        (index, shares, hidden, expert_ids.T),
        smem=(0,),
        scratch=(wide,),
        leave=(1,),
    )
    payload, later, when = together(payload, middle, index)
    arrived = exchange(payload, "ep")
    width = w_expert_gate.shape[2]
    packed, down = call(
        pack_body,
        (shape((MODEL_WIDTH + 4 * width, 2 * width), BF16), shape((4 * width, 2 * width), BF16)),
        (when, w_expert_gate, w_expert_up, w_expert_down),
        smem=(0,),
        raw=(1, 2, 3),
        scratch=(pltpu.SemaphoreType.DMA((2 + 2 * chips,)),),
    )
    away = core_swap(packed)
    arrived, packed, down, away = together(arrived, packed, down, away)
    payload = call(
        expert_body,
        large,
        (
            index,
            arrived,
            core_swap(arrived),
            ffn_gain,
            packed,
            down,
            away,
        ),
        smem=(0,),
        leave=(0,),
        scratch=(
            wide,
            wide,
            pltpu.VMEM((slots, MODEL_WIDTH), BF16),
            pltpu.VMEM((1, MODEL_WIDTH), F32),
        ),
    )
    payload, later = together(payload, later)
    returned = exchange(payload, "ep")
    other_half = core_swap(later)
    side_weights = (
        ffn_gain,
        dense_gate,
        w_shared_gate.T,
        w_shared_up.T,
        w_dense_up,
        w_shared_down,
        w_dense_down,
    )
    side, away = call(
        side_body,
        (shape(half, F32), shape(half, F32)),
        (
            index,
            later,
            other_half,
            *side_weights,
        ),
        smem=(0,),
        raw=range(3, 10),
        leave=(1,),
        scratch=(
            *(pltpu.VMEM(w.shape, BF16) for w in side_weights),
            pltpu.SemaphoreType.DMA((len(side_weights),)),
        ),
    )
    away = core_swap(away)
    returned, side = together(returned, side + away)

    payload = call(
        combine_body,
        shape((chips, tokens, LANES), BF16),
        (returned, combine, side),
        scratch=(wide,),
    )
    parts = exchange(payload, "tp", same_core)
    return call(
        final_body, shape((tokens, LANES), BF16), (index, parts, middle), smem=(0,), leave=(0,)
    )


def solution(mesh):
    placed = (
        P("ep", None),
        P(("ep", "tp")),
        P(("ep", "tp"), None, None),
        P(("ep", "tp"), None, None),
        P(),
        P(None, "tp"),
        P(None, "tp"),
        P(),
        P(),
        P(),
        P("tp", None),
        P(None, "tp"),
        P("tp"),
        P("tp", None),
        P(),
        P("ep", None),
        P("ep", None),
        P("ep", None, "tp"),
        P("ep", None, "tp"),
        P("ep", "tp", None),
        P(None, "tp"),
        P(None, "tp"),
        P("tp", None),
        P(None, "tp"),
        P("tp", None),
        P(),
    )
    return jax.shard_map(
        on_device, mesh=mesh, in_specs=placed, out_specs=P("ep", "tp"), check_vma=False
    )
```
